512 devices in a mesh: fs: 64 (over z, y), tp: 8 (over x, core).
Axes of the slice: x: 4, y: 8, z: 8, core: 2. Of those that a mesh axis runs over, the one named last changes fastest.
Arguments:
- tokens: bfloat16 [24576, 2048], P('fs', 'tp'), may hold values from -6 to 6
- outer_gate: bfloat16 [2048, 2048], P('fs', 'tp'), may hold values from -0.125 to 0.125
- inner_gate: bfloat16 [2048, 2048], P('fs', 'tp'), may hold values from -0.125 to 0.125
- mix_value: bfloat16 [2048, 2048], P('fs', 'tp'), may hold values from -0.125 to 0.125
- mix_taps: bfloat16 [3, 2048], P(None, 'tp'), may hold values from -3 to 3
- mix_out: bfloat16 [2048, 2048], P('tp', 'fs'), may hold values from -0.375 to 0.375
- mix_gain: bfloat16 [2048], P('tp'), may hold values from 0.099609375 to 1.8984375
- ffn_gate: bfloat16 [2048, 3072], P('fs', 'tp'), may hold values from -0.125 to 0.125
- ffn_value: bfloat16 [2048, 3072], P('fs', 'tp'), may hold values from -0.125 to 0.125
- gate_taps: bfloat16 [3, 3072], P(None, 'tp'), may hold values from -3 to 3
- value_taps: bfloat16 [3, 3072], P(None, 'tp'), may hold values from -3 to 3
- ffn_down: bfloat16 [3072, 2048], P('tp', 'fs'), may hold values from -0.3125 to 0.3125
- ffn_gain: bfloat16 [2048], P('tp'), may hold values from 0.099609375 to 1.8984375
Outputs:
- layer_out: bfloat16 [24576, 2048], P('fs', 'tp')
The draws below stay inside these ranges and needn't reach their ends.
All inputs are finite; a program needn't handle non-finite values.
Results may differ from the reference program's by a relative error of at most 0.015.
Values may be sent and summed in bfloat16 or wider, within the bound.
A program may use at most 64 MiB of HBM per device.

```python
import jax
import jax.numpy as jnp
from jax import lax

D = 2048
F = 3072
SEQ_LEN = 128
TOKENS = 24576
N_TP = 8


def with_spikes(values, own_key, source, target, blocks, factor):
    def block_of(dim):
        return (jnp.arange(values.shape[dim]) // (values.shape[dim] // blocks)).reshape((-1,) + (1,) * (values.ndim - 1 - dim))

    one_side = jax.random.permutation(own_key, blocks)[block_of(target)]
    far = (block_of(target) + blocks // 2) % blocks
    return jnp.where((block_of(source) == one_side) | (block_of(source) == far), factor * values, values)


def shard_levels(key, shape, pieces, smallest, high):
    loudness = 1.0
    for axis_at, shards_of in pieces:
        heights = jax.random.uniform(jax.random.fold_in(jax.random.fold_in(key, 6), axis_at), (shards_of,), jnp.float32, smallest / len(pieces), high / len(pieces))
        loudness = loudness * jnp.repeat(jnp.exp(heights), shape[axis_at] // shards_of).reshape((-1,) + (1,) * (len(shape) - 1 - axis_at))
    return loudness


def noise(stream_key, extent, scale, most, pieces=(), kind=jnp.bfloat16):
    values = jax.random.normal(stream_key, extent, jnp.float32) * scale
    if len(pieces) > 0:
        values = shard_levels(stream_key, extent, pieces, -0.22, 0.18) * values
    return jnp.clip(values, min=-most, max=most).astype(kind)


def heavy_noise(stream_key, extent, deviation, bound, cuts, heavy, kind=jnp.bfloat16):
    drawn = deviation * jax.random.normal(stream_key, extent, jnp.float32)
    if cuts:
        drawn = drawn * shard_levels(stream_key, extent, cuts, -0.22, 0.18)
    return jnp.clip(with_spikes(drawn, jax.random.fold_in(stream_key, 3), *heavy), -bound, bound).astype(kind)


def setup_inputs(seed: int = 0) -> dict:
    streams_of = jax.random.split(jax.random.key(seed), 14)
    return {
        "tokens": noise(streams_of[0], (TOKENS, D), 1.0, 6.0, ((0, 64), (1, 8))),
        "outer_gate": noise(streams_of[1], (D, D), D ** -0.5, 0.125, ((0, 64), (1, 8))),
        "inner_gate": noise(streams_of[2], (D, D), D ** -0.5, 0.125, ((0, 64), (1, 8))),
        "mix_value": noise(streams_of[3], (D, D), D ** -0.5, 0.125, ((0, 64), (1, 8))),
        "mix_taps": noise(streams_of[4], (3, D), 0.577, 3.0, ((1, 8),)),
        "mix_out": heavy_noise(streams_of[5], (D, D), D ** -0.5, 0.375, ((0, 8), (1, 64)), (0, 1, 64, 4.0)),
        "mix_gain": jnp.clip(1.0 + 0.18 * jax.random.normal(streams_of[6], (D,), jnp.float32), 0.099609375, 1.8984375).astype(jnp.bfloat16),
        "ffn_gate": noise(streams_of[7], (D, F), D ** -0.5, 0.125, ((0, 64), (1, 8))),
        "ffn_value": noise(streams_of[8], (D, F), D ** -0.5, 0.125, ((0, 64), (1, 8))),
        "gate_taps": noise(streams_of[9], (3, F), 0.577, 3.0, ((1, 8),)),
        "value_taps": noise(streams_of[10], (3, F), 0.577, 3.0, ((1, 8),)),
        "ffn_down": heavy_noise(streams_of[11], (F, D), F ** -0.5, 0.3125, ((0, 8), (1, 64)), (0, 1, 64, 4.0)),
        "ffn_gain": jnp.clip(1.0 + 0.18 * jax.random.normal(streams_of[12], (D,), jnp.float32), 0.099609375, 1.8984375).astype(jnp.bfloat16),
    }


residual_scale = 8.0 ** 0.25
norm_epsilon = 1e-05

def stored(values):
    return lax.optimization_barrier(values.astype(jnp.bfloat16)).astype(jnp.float32)

def shift_rows(values, offset):
    position = jnp.arange(values.shape[0]) % SEQ_LEN
    shifted = jnp.concatenate([jnp.zeros((offset, values.shape[1]), values.dtype), values[:-offset]], axis=0)
    return jnp.where((position >= offset)[:, None], shifted, jnp.zeros_like(shifted))

def causal_taps(values, taps):
    weights = taps.astype(jnp.float32)
    return values * weights[2] + shift_rows(values, 1) * weights[1] + shift_rows(values, 2) * weights[0]

def norm_rows(hidden, gain):
    mean = lax.optimization_barrier(jnp.mean(hidden, axis=1, keepdims=True))
    spread = lax.optimization_barrier(jnp.mean(jnp.square(hidden - mean), axis=1, keepdims=True))
    return ((hidden - mean) * lax.rsqrt(spread + norm_epsilon) * gain.astype(jnp.float32)).astype(jnp.bfloat16)

def split_sum(left, right):
    width = left.shape[1] // N_TP
    total = jnp.zeros((left.shape[0], right.shape[1]), jnp.float32)
    for index in range(N_TP):
        term = jnp.dot(left[:, index * width:(index + 1) * width], right[index * width:(index + 1) * width], preferred_element_type=jnp.float32)
        total = total + stored(term)
    return total

def reference(tokens, outer_gate, inner_gate, mix_value, mix_taps, mix_out, mix_gain, ffn_gate, ffn_value, gate_taps, value_taps, ffn_down, ffn_gain):
    outer = stored(jnp.dot(tokens, outer_gate, preferred_element_type=jnp.float32))
    inner = stored(jnp.dot(tokens, inner_gate, preferred_element_type=jnp.float32))
    values = stored(jnp.dot(tokens, mix_value, preferred_element_type=jnp.float32))
    gated = (outer * causal_taps(inner * values, mix_taps)).astype(jnp.bfloat16)
    mixer_branch = split_sum(gated, mix_out)
    first = norm_rows(residual_scale * tokens.astype(jnp.float32) + mixer_branch, mix_gain)
    gate_up = stored(jnp.dot(first, ffn_gate, preferred_element_type=jnp.float32))
    value_up = stored(jnp.dot(first, ffn_value, preferred_element_type=jnp.float32))
    hidden = (jax.nn.silu(causal_taps(gate_up, gate_taps)) * causal_taps(value_up, value_taps)).astype(jnp.bfloat16)
    ffn_branch = split_sum(hidden, ffn_down)
    return norm_rows(residual_scale * first.astype(jnp.float32) + ffn_branch, ffn_gain)
```

```python
import functools

import jax
import jax.numpy as jnp
from jax import lax
from jax.experimental import pallas as pl
from jax.experimental.pallas import tpu as pltpu
from jax.sharding import PartitionSpec as P

SEQ_LEN = 128
RING_Z = 8
RING_Y = 8
residual_scale = 8.0**0.25
norm_epsilon = 1e-05
MESH = pl.DeviceIdType.MESH
RIGHT, LEFT = 0, 1
VMEM_LIMIT = 60 * 1024 * 1024
F32 = jnp.float32
BF16 = jnp.bfloat16


def nt_dot(a, b):
    return lax.dot_general(a, b, (((1,), (1,)), ((), ())), preferred_element_type=F32)


def kernel(
    cfg,
    tok_ref,
    og_ref,
    ig_ref,
    mv_ref,
    mtaps_ref,
    mo_ref,
    mgain_ref,
    fg_ref,
    fv_ref,
    gtaps_ref,
    vtaps_ref,
    fd_ref,
    fgain_ref,
    out_ref,
    g1,
    g2,
    g3,
    g4,
    tokw,
    gainw,
    proj,
    gated,
    ppart_m,
    pown_m,
    dbuf_m,
    sbuf_m,
    rbuf_m,
    branchw,
    firstw,
    up,
    hidden,
    ppart_f,
    pown_f,
    dbuf_f,
    sbuf_f,
    rbuf_f,
    ybuf,
    stats,
    mtapf,
    gtapf,
    vtapf,
    wsend,
    wrecv,
    loc_sem,
    tok_send,
    tok_recv,
    gain_send,
    gain_recv,
    d_send,
    d_recv,
    x_send,
    x_recv,
    ag_send,
    ag_recv,
    fw_send,
    st_send,
    st_recv,
):
    Z, Y, TP = cfg
    X = TP // 2
    rows, dl = tok_ref.shape
    kr = og_ref.shape[0]
    h = kr // 2
    fl = fg_ref.shape[1]
    D = TP * dl
    fs = lax.axis_index("fs")
    tp = lax.axis_index("tp")
    z, y = fs // Y, fs % Y
    x, c = tp // 2, tp % 2
    partner = 2 * x + (1 - c)
    gs = (g1, g2, g3, g4)

    def ring_id(axis, step):
        if axis == "y":
            return (z * Y + (y + step + Y) % Y, tp)
        return (((z + step + Z) % Z) * Y + y, tp)

    def block(ref, b):
        return ref.at[:, pl.ds(pl.multiple_of(b * dl, dl), dl)]

    local = []

    def place(src, dst):
        copy = pltpu.make_async_copy(src, dst, loc_sem.at[len(local)])
        copy.start()
        local.append(copy)

    for i, ref in enumerate((og_ref, ig_ref, mv_ref)):
        for half in range(2):
            place(ref.at[pl.ds(half * h, h)], g1.at[z, y, half, :, pl.ds(i * dl, dl)])
    for i, ref in enumerate((fg_ref, fv_ref)):
        for half in range(2):
            place(ref.at[pl.ds(half * h, h)], g3.at[z, y, half, :, pl.ds(i * fl, fl)])
    place(tok_ref, block(tokw, tp))

    barrier = pltpu.get_barrier_semaphore()
    for axis in ("y", "z"):
        for step in (1, -1):
            pl.semaphore_signal(barrier, inc=1, device_id=ring_id(axis, step), device_id_type=MESH)
    for d in range(1, TP):
        pl.semaphore_signal(barrier, inc=1, device_id=(fs, (tp + d) % TP), device_id_type=MESH)

    eye = (
        lax.broadcasted_iota(jnp.int32, (kr, kr), 0) == lax.broadcasted_iota(jnp.int32, (kr, kr), 1)
    ).astype(BF16)
    for g, ref in ((g2, mo_ref), (g4, fd_ref)):
        turned = nt_dot(eye, ref[...]).astype(BF16)
        g[z, y, 0] = turned[:h]
        g[z, y, 1] = turned[h:]
    gainw[:, pl.ds(pl.multiple_of(tp * dl, dl), dl)] = jnp.broadcast_to(mgain_ref[...].astype(F32), (8, dl))
    mtapf[...] = mtaps_ref[...].astype(F32)
    gtapf[...] = gtaps_ref[...].astype(F32)
    vtapf[...] = vtaps_ref[...].astype(F32)
    for copy in local:
        copy.wait()
    pl.semaphore_wait(barrier, 4 + TP - 1)

    def piece(w, colour, phase, origin, half):
        g = gs[w]
        cols = g.shape[-1]
        cut = (cols // 128 + 1) // 2 * 128
        if phase == 0:
            lead = (z, origin, 0) if colour == 0 else (origin, y, 1)
            if half is None:
                return g.at[lead]
            span = pl.ds(0, cut) if half == 0 else pl.ds(cut, cols - cut)
            return g.at[(*lead, slice(None), span)]
        across = Y if colour == 0 else Z
        span = pl.ds(0, across) if half is None else pl.ds(half * (across // 2), across // 2)
        return g.at[origin, span, 0] if colour == 0 else g.at[span, origin, 1]

    def weight_copy(w, colour, phase, way, step, incoming=False):
        along_y = (colour == 0) == (phase == 0)
        axis, n, me = ("y", Y, y) if along_y else ("z", Z, z)
        last = step == n // 2 - 1
        half = way if last else None
        shift = -step if way == RIGHT else step
        if incoming:
            shift = shift - 1 if way == RIGHT else shift + 1
        origin = (me + shift + n) % n
        ref = piece(w, colour, phase, origin, half)
        at = (((w * 2 + colour) * 2 + phase) * 2 + way) * 4 + step
        return pltpu.make_async_remote_copy(
            src_ref=ref,
            dst_ref=ref,
            send_sem=wsend.at[at],
            recv_sem=wrecv.at[at],
            device_id=ring_id(axis, 1 if way == RIGHT else -1),
            device_id_type=MESH,
        )

    sent = []

    def steps_of(colour, phase):
        return (Y if (colour == 0) == (phase == 0) else Z) // 2

    def send_weights(w, phase, step):
        for colour in range(2):
            if step < steps_of(colour, phase):
                for way in (RIGHT, LEFT):
                    copy = weight_copy(w, colour, phase, way, step)
                    copy.start()
                    sent.append(copy)

    def pass_on(w, phase, step):
        for colour in range(2):
            for way in (RIGHT, LEFT):
                if step < steps_of(colour, phase):
                    weight_copy(w, colour, phase, way, step, incoming=True).wait_recv()
                if step + 1 < steps_of(colour, phase):
                    copy = weight_copy(w, colour, phase, way, step + 1)
                    copy.start()
                    sent.append(copy)

    def to_tp(src, dst, send_sem, recv_sem, peer):
        return pltpu.make_async_remote_copy(
            src_ref=src, dst_ref=dst, send_sem=send_sem, recv_sem=recv_sem, device_id=(fs, peer), device_id_type=MESH
        )

    most = max(Y, Z) // 2
    send_weights(0, 0, 0)
    send_weights(1, 0, 0)
    for d in range(1, TP):
        peer = (tp + d) % TP
        mine = block(tokw, tp)
        copy = to_tp(mine, mine, tok_send.at[d], tok_recv.at[d], peer)
        copy.start()
        sent.append(copy)
        mine = block(gainw, tp)
        copy = to_tp(mine, mine, gain_send.at[d], gain_recv.at[d], peer)
        copy.start()
        sent.append(copy)
    send_weights(2, 0, 0)
    send_weights(3, 0, 0)
    for step in range(most):
        for w in range(4):
            pass_on(w, 0, step)
            if step == most - 1 and w < 2:
                send_weights(w, 1, 0)
    for step in range(most):
        for w in range(2):
            if step == most - 1 and w == 0:
                send_weights(2, 1, 0)
                send_weights(3, 1, 0)
            pass_on(w, 1, step)
    for d in range(1, TP):
        peer = (tp - d + TP) % TP
        theirs = block(tokw, peer)
        to_tp(theirs, theirs, tok_send.at[d], tok_recv.at[d], peer).wait_recv()
        theirs = block(gainw, peer)
        to_tp(theirs, theirs, gain_send.at[d], gain_recv.at[d], peer).wait_recv()

    def taps_of(v, tap_ref, cols):
        at = lax.broadcasted_iota(jnp.int32, v.shape, 0)
        one = jnp.where(at >= 1, pltpu.roll(v, 1, 0), 0.0)
        two = jnp.where(at >= 2, pltpu.roll(v, 2, 0), 0.0)
        return v * tap_ref[2:3, cols] + one * tap_ref[1:2, cols] + two * tap_ref[0:1, cols]

    n_seq = rows // SEQ_LEN

    def tiles(cols, body):
        across = cols // 128

        def one(i, carry):
            r = pl.ds(pl.multiple_of((i // across) * SEQ_LEN, SEQ_LEN), SEQ_LEN)
            body(r, pl.multiple_of((i % across) * 128, 128))
            return carry

        lax.fori_loop(0, n_seq * across, one, 0)

    def whole_rows(g, first_col, cols):
        return g[:, :, :, :, pl.ds(first_col, cols)].reshape(D, cols)

    def project(left, g, target):
        def one(n, carry):
            at = pl.multiple_of(n * 256, 256)
            target[:, pl.ds(at, 256)] = jnp.dot(
                left[...], whole_rows(g, at, 256), preferred_element_type=F32
            ).astype(BF16)
            return carry

        lax.fori_loop(0, g.shape[-1] // 256, one, 0)

    def reduce_start(slot, left, g, ppart, pown, dbuf):
        def theirs(j, carry):
            rhs = g[2 * j + 1 - c].reshape(dl, g.shape[-1])
            ppart[j] = nt_dot(left[...], rhs).astype(BF16)
            to_tp(ppart.at[j], dbuf.at[j], d_send.at[slot, j], d_recv.at[slot, j], partner).start()
            return carry

        lax.fori_loop(0, X, theirs, 0)

        def ours(j, carry):
            rhs = g[2 * j + c].reshape(dl, g.shape[-1])
            pown[j] = nt_dot(left[...], rhs).astype(BF16)
            return carry

        lax.fori_loop(0, X, ours, 0)

    def d_wait(slot, j, ppart, dbuf):
        to_tp(ppart.at[j], dbuf.at[j], d_send.at[slot, j], d_recv.at[slot, j], partner).wait()

    away = [d for d in (X // 2, *range(1, X)) if d > 0]
    away = list(dict.fromkeys(away))

    def reduce_cross(slot, ppart, pown, dbuf, sbuf, rbuf):
        for d in away:
            j = (x + d) % X
            d_wait(slot, j, ppart, dbuf)
            sbuf[d] = (pown[j].astype(F32) + dbuf[j].astype(F32)).astype(BF16)
            copy = to_tp(sbuf.at[d], rbuf.at[d], x_send.at[slot, d], x_recv.at[slot, d], 2 * j + c)
            copy.start()
            sent.append(copy)
        d_wait(slot, x, ppart, dbuf)

    def reduce_end(slot, pown, dbuf, sbuf, rbuf):
        for d in away:
            to_tp(sbuf.at[d], rbuf.at[d], x_send.at[slot, d], x_recv.at[slot, d], 2 * ((x - d + X) % X) + c).wait_recv()

        def total(r):
            acc = pown[x, r].astype(F32) + dbuf[x, r].astype(F32)
            for d in away:
                acc = acc + rbuf[d, r].astype(F32)
            return acc

        return total

    project(tokw, g1, proj)

    def mix(r, at):
        cols = pl.ds(at, 128)
        outer = proj[r, cols].astype(F32)
        inner = proj[r, pl.ds(pl.multiple_of(dl + at, 128), 128)].astype(F32)
        value = proj[r, pl.ds(pl.multiple_of(2 * dl + at, 128), 128)].astype(F32)
        gated[r, cols] = (outer * taps_of(inner * value, mtapf, cols)).astype(BF16)

    tiles(dl, mix)
    reduce_start(0, gated, g2, ppart_m, pown_m, dbuf_m)
    reduce_cross(0, ppart_m, pown_m, dbuf_m, sbuf_m, rbuf_m)
    for step in range(min(2, most - 1)):
        for w in (2, 3):
            pass_on(w, 1, step)
    total = reduce_end(0, pown_m, dbuf_m, sbuf_m, rbuf_m)
    own_cols = pl.ds(pl.multiple_of(tp * dl, dl), dl)
    for s in range(n_seq):
        r = pl.ds(s * SEQ_LEN, SEQ_LEN)
        branchw[r, own_cols] = total(r).astype(BF16)
    mine = block(branchw, tp)
    for d in away:
        copy = to_tp(mine, mine, ag_send.at[d], ag_recv.at[tp], 2 * ((x + d) % X) + c)
        copy.start()
        sent.append(copy)
    copy = to_tp(mine, mine, ag_send.at[0], ag_recv.at[tp], partner)
    copy.start()
    sent.append(copy)
    for step in range(2, most - 1):
        for w in (2, 3):
            pass_on(w, 1, step)
    for d in away:
        b = 2 * ((x - d + X) % X) + c
        theirs = block(branchw, b)
        to_tp(theirs, theirs, ag_send.at[d], ag_recv.at[b], b).wait_recv()
        copy = to_tp(theirs, theirs, fw_send.at[d], ag_recv.at[b], partner)
        copy.start()
        sent.append(copy)
    for d in [0, *away]:
        b = 2 * ((x - d + X) % X) + 1 - c
        theirs = block(branchw, b)
        to_tp(theirs, theirs, ag_send.at[d], ag_recv.at[b], partner).wait_recv()

    def norm_first(i, carry):
        r = pl.ds(pl.multiple_of(i * 16, 16), 16)
        v = residual_scale * tokw[r, :].astype(F32) + branchw[r, :].astype(F32)
        mean = jnp.sum(v, axis=1, keepdims=True) * (1.0 / D)
        v = v - mean
        spread = jnp.sum(v * v, axis=1, keepdims=True) * (1.0 / D)
        firstw[r, :] = (v * lax.rsqrt(spread + norm_epsilon) * gainw[0:1, :]).astype(BF16)
        return carry

    lax.fori_loop(0, rows // 16, norm_first, 0)

    pass_on(2, 1, most - 1)
    project(firstw, g3, up)

    def gate(r, at):
        cols = pl.ds(at, 128)
        left = taps_of(up[r, cols].astype(F32), gtapf, cols)
        right = taps_of(up[r, pl.ds(pl.multiple_of(fl + at, 128), 128)].astype(F32), vtapf, cols)
        hidden[r, cols] = (left / (1.0 + jnp.exp(-left)) * right).astype(BF16)

    tiles(fl, gate)
    pass_on(3, 1, most - 1)
    reduce_start(1, hidden, g4, ppart_f, pown_f, dbuf_f)
    reduce_cross(1, ppart_f, pown_f, dbuf_f, sbuf_f, rbuf_f)
    total = reduce_end(1, pown_f, dbuf_f, sbuf_f, rbuf_f)
    lane = lax.broadcasted_iota(jnp.int32, (SEQ_LEN, 128), 1)
    for s in range(n_seq):
        r = pl.ds(s * SEQ_LEN, SEQ_LEN)
        v = residual_scale * firstw[r, own_cols].astype(F32) + total(r)
        ybuf[r, :] = v
        mean = jnp.sum(v, axis=1, keepdims=True) * (1.0 / dl)
        v = v - mean
        square = jnp.sum(v * v, axis=1, keepdims=True)
        both = jnp.where(lane == 0, mean, jnp.where(lane == 1, square, 0.0))
        stats[tp, :, s * SEQ_LEN : (s + 1) * SEQ_LEN] = both.T[:8]
    for d in range(1, TP):
        copy = to_tp(stats.at[tp], stats.at[tp], st_send.at[d], st_recv.at[d], (tp + d) % TP)
        copy.start()
        sent.append(copy)
    for d in range(1, TP):
        b = (tp - d + TP) % TP
        to_tp(stats.at[b], stats.at[b], st_send.at[d], st_recv.at[d], b).wait_recv()
    row8 = lax.broadcasted_iota(jnp.int32, (128, SEQ_LEN), 0)
    for s in range(n_seq):
        r = pl.ds(s * SEQ_LEN, SEQ_LEN)
        theirs = stats[:, :, s * SEQ_LEN : (s + 1) * SEQ_LEN]
        means, squares = theirs[:, 0], theirs[:, 1]
        mean = jnp.sum(means, axis=0, keepdims=True) * (1.0 / TP)
        off = means - mean
        spread = (jnp.sum(squares, axis=0, keepdims=True) + dl * jnp.sum(off * off, axis=0, keepdims=True)) * (1.0 / D)
        scale = lax.rsqrt(spread + norm_epsilon)
        both = jnp.where(row8 == 0, mean, jnp.where(row8 == 1, scale, 0.0)).T
        v = (ybuf[r, :] - both[:, 0:1]) * both[:, 1:2]
        out_ref[r, :] = (v * fgain_ref[...].astype(F32)).astype(BF16)
    for copy in sent:
        copy.wait_send()


def layer(cfg, tokens, outer_gate, inner_gate, mix_value, mix_taps, mix_out, mix_gain, ffn_gate, ffn_value, gate_taps, value_taps, ffn_down, ffn_gain):
    Z, Y, TP = cfg
    X = TP // 2
    rows, dl = tokens.shape
    kr = outer_gate.shape[0]
    h = kr // 2
    fl = ffn_gate.shape[1]
    D = TP * dl
    ring = 4 * 2 * 2 * 2 * 4
    vmem = pl.BlockSpec(memory_space=pltpu.VMEM)
    hbm = pl.BlockSpec(memory_space=pl.ANY)
    dma = pltpu.SemaphoreType.DMA
    blocks = [
        pltpu.VMEM((X, rows, dl), BF16),
        pltpu.VMEM((X, rows, dl), BF16),
        pltpu.VMEM((X, rows, dl), BF16),
        pltpu.VMEM((X, rows, dl), BF16),
        pltpu.VMEM((X, rows, dl), BF16),
    ]
    return pl.pallas_call(
        functools.partial(kernel, cfg),
        out_shape=jax.ShapeDtypeStruct((rows, dl), BF16),
        in_specs=[hbm, hbm, hbm, hbm, vmem, vmem, vmem, hbm, hbm, vmem, vmem, vmem, vmem],
        out_specs=vmem,
        scratch_shapes=[
            pltpu.VMEM((Z, Y, 2, h, 3 * dl), BF16),
            pltpu.VMEM((Z, Y, 2, h, dl), BF16),
            pltpu.VMEM((Z, Y, 2, h, 2 * fl), BF16),
            pltpu.VMEM((Z, Y, 2, h, fl), BF16),
            pltpu.VMEM((rows, D), BF16),
            pltpu.VMEM((8, D), F32),
            pltpu.VMEM((rows, 3 * dl), BF16),
            pltpu.VMEM((rows, dl), BF16),
            *blocks,
            pltpu.VMEM((rows, D), BF16),
            pltpu.VMEM((rows, D), BF16),
            pltpu.VMEM((rows, 2 * fl), BF16),
            pltpu.VMEM((rows, fl), BF16),
            *blocks,
            pltpu.VMEM((rows, dl), F32),
            pltpu.VMEM((TP, 8, rows), F32),
            pltpu.VMEM((3, dl), F32),
            pltpu.VMEM((3, fl), F32),
            pltpu.VMEM((3, fl), F32),
            dma((ring,)),
            dma((ring,)),
            dma((11,)),
            dma((TP,)),
            dma((TP,)),
            dma((TP,)),
            dma((TP,)),
            dma((2, X)),
            dma((2, X)),
            dma((2, X)),
            dma((2, X)),
            dma((X,)),
            dma((TP,)),
            dma((X,)),
            dma((TP,)),
            dma((TP,)),
        ],
        compiler_params=pltpu.CompilerParams(
            collective_id=0, has_side_effects=True, vmem_limit_bytes=VMEM_LIMIT
        ),
    )(
        tokens,
        outer_gate,
        inner_gate,
        mix_value,
        mix_taps,
        mix_out,
        mix_gain.reshape(1, dl),
        ffn_gate,
        ffn_value,
        gate_taps,
        value_taps,
        ffn_down,
        ffn_gain.reshape(1, dl),
    )


def solution(mesh):
    placed = (
        P("fs", "tp"),
        P("fs", "tp"),
        P("fs", "tp"),
        P("fs", "tp"),
        P(None, "tp"),
        P("tp", "fs"),
        P("tp"),
        P("fs", "tp"),
        P("fs", "tp"),
        P(None, "tp"),
        P(None, "tp"),
        P("tp", "fs"),
        P("tp"),
    )
    cfg = (RING_Z, RING_Y, mesh.shape["tp"])
    return jax.shard_map(
        functools.partial(layer, cfg), mesh=mesh, in_specs=placed, out_specs=P("fs", "tp"), check_vma=False
    )
```

```python
import functools

import jax
import jax.numpy as jnp
from jax import lax
from jax.experimental import pallas as pl
from jax.experimental.pallas import tpu as pltpu
from jax.sharding import PartitionSpec as P

SEQ_LEN = 128
RING_Z = 8
RING_Y = 8
residual_scale = 8.0**0.25
norm_epsilon = 1e-05
MESH = pl.DeviceIdType.MESH
RIGHT, LEFT = 0, 1
LATE = 2
LATE_AT = {
    2: ("mixer", 2),
    3: ("gather_start", 0),
    4: ("gather_start", 1),
    5: ("gather_share", 0),
    6: ("gather_share", 1),
    7: ("gather_share", 2),
    8: None,
}
VMEM_LIMIT = 60 * 1024 * 1024
F32 = jnp.float32
BF16 = jnp.bfloat16


def nt_dot(a, b):
    return lax.dot_general(a, b, (((1,), (1,)), ((), ())), preferred_element_type=F32)


def kernel(
    cfg,
    tok_ref,
    og_ref,
    ig_ref,
    mv_ref,
    mtaps_ref,
    mo_ref,
    mgain_ref,
    fg_ref,
    fv_ref,
    gtaps_ref,
    vtaps_ref,
    fd_ref,
    fgain_ref,
    out_ref,
    g12,
    g34,
    tokw,
    gainw,
    branchw,
    firstw,
    normed,
    proj,
    gated,
    up,
    hidden,
    ppart_m,
    pown_m,
    dbuf_m,
    sbuf_m,
    rbuf_m,
    ppart_f,
    pown_f,
    dbuf_f,
    sbuf_f,
    rbuf_f,
    ybuf,
    stats,
    mtapf,
    gtapf,
    vtapf,
    wrecv,
    wsend,
    loc_sem,
    tok_sem,
    gain_sem,
    dsend,
    drecv,
    xsend,
    xrecv,
    agx_send,
    agx_recv,
    agd_send,
    agd_recv,
    st_send,
    st_recv,
):
    Z, Y, TP = cfg
    X = TP // 2
    rows, dl = tok_ref.shape
    kr = og_ref.shape[0]
    h = kr // 2
    fl = fg_ref.shape[1]
    D = TP * dl
    n_seq = rows // SEQ_LEN
    fs = lax.axis_index("fs")
    tp = lax.axis_index("tp")
    z, y = fs // Y, fs % Y
    x, c = tp // 2, tp % 2
    partner = 2 * x + (1 - c)
    groups = (g12, g34)
    away = list(dict.fromkeys([X // 2, *range(1, X)]))

    def ring_id(axis, step):
        if axis == "y":
            return (z * Y + (y + step + Y) % Y, tp)
        return (((z + step + Z) % Z) * Y + y, tp)

    def span(at, size):
        return pl.ds(pl.multiple_of(at, size), size)

    def remote(src, dst, send_sem, recv_sem, to):
        return pltpu.make_async_remote_copy(
            src_ref=src, dst_ref=dst, send_sem=send_sem, recv_sem=recv_sem, device_id=to, device_id_type=MESH
        )

    def await_recv(box, sem):
        remote(box, box, sem, sem, (fs, partner)).wait_recv()

    def await_send(box, sem):
        remote(box, box, sem, sem, (fs, partner)).wait_send()

    barrier = pltpu.get_barrier_semaphore()
    for axis in ("y", "z"):
        for step in (1, -1):
            pl.semaphore_signal(barrier, inc=1, device_id=ring_id(axis, step), device_id_type=MESH)
    for d in range(1, TP):
        pl.semaphore_signal(barrier, inc=1, device_id=(fs, (tp + d) % TP), device_id_type=MESH)

    def place(g, refs, sem):
        at = 0
        for ref in refs:
            cols = ref.shape[1]
            for half in range(2):
                pltpu.make_async_copy(
                    ref.at[pl.ds(half * h, h)], g.at[z, y, half, :, pl.ds(at, cols)], sem
                ).start()
            at += cols

    own_tokens = pltpu.make_async_copy(tok_ref, tokw.at[:, span(tp * dl, dl)], loc_sem.at[2])
    place(g12, (og_ref, ig_ref, mv_ref, mo_ref), loc_sem.at[0])
    own_tokens.start()
    place(g34, (fg_ref, fv_ref, fd_ref), loc_sem.at[1])
    gainw[:, span(tp * dl, dl)] = jnp.broadcast_to(mgain_ref[...].astype(F32).reshape(1, dl), (8, dl))
    mtapf[...] = mtaps_ref[...].astype(F32)
    gtapf[...] = gtaps_ref[...].astype(F32)
    vtapf[...] = vtaps_ref[...].astype(F32)
    for i, g in enumerate(groups):
        pltpu.make_async_copy(g.at[z, y], g.at[z, y], loc_sem.at[i]).wait()
    own_tokens.wait()
    with jax.named_scope("greet"):
        pl.semaphore_wait(barrier, 4 + TP - 1)

    def piece(w, colour, one, two):
        return groups[w].at[two, one, 0] if colour == 0 else groups[w].at[one, two, 1]

    def rings(colour):
        return (("y", Y, y), ("z", Z, z)) if colour == 0 else (("z", Z, z), ("y", Y, y))

    def recv_sem(w, colour, kind, step):
        return wrecv.at[((w * 2 + colour) * 6 + kind) * 4 + step]

    def send_first(w, colour, step):
        (axis, n, me), (_, _, other) = rings(colour)
        for way in (RIGHT, LEFT):
            if step == n // 2 - 1 and way != w % 2:
                continue
            origin = (me - step + n) % n if way == RIGHT else (me + step) % n
            ref = piece(w, colour, origin, other)
            remote(
                ref, ref, wsend.at[2 * w], recv_sem(w, colour, 5, step), ring_id(axis, 1 if way == RIGHT else -1)
            ).start()

    def first_count(colour, step):
        return 1 if step == rings(colour)[0][1] // 2 - 1 else 2

    def members(n, g):
        return [0] if g == 0 else [g] if g == n // 2 else [g, -g]

    def halves(n, g):
        return ([0], []) if g == 0 else ([], [g]) if g == n // 2 else ([g], [-g])

    def send_second(w, colour, g, step):
        (_, n1, me1), (axis, n2, me2) = rings(colour)
        for way in (RIGHT, LEFT):
            at = members(n1, g) if step < n2 // 2 - 1 else halves(n1, g)[way]
            origin = (me2 - step + n2) % n2 if way == RIGHT else (me2 + step) % n2
            for m in at:
                ref = piece(w, colour, (me1 + m + n1) % n1, origin)
                remote(
                    ref, ref, wsend.at[2 * w + 1], recv_sem(w, colour, g, step), ring_id(axis, 1 if way == RIGHT else -1)
                ).start()

    def second_count(colour, g, step):
        n1, n2 = rings(colour)[0][1], rings(colour)[1][1]
        if step < n2 // 2 - 1:
            return 2 * len(members(n1, g))
        return sum(len(part) for part in halves(n1, g))

    def await_pieces(w, count, sem):
        g = groups[w]
        await_recv(g.at[0, 0, 0] if count == 1 else g.at[pl.ds(0, count), 0, 0], sem)

    def begin(w):
        for colour in range(2):
            send_first(w, colour, 0)
        for colour in range(2):
            send_second(w, colour, 0, 0)

    def tick(w, k):
        for colour in range(2):
            n1 = rings(colour)[0][1]
            if 0 <= k < n1 // 2:
                await_pieces(w, first_count(colour, k), recv_sem(w, colour, 5, k))
                if k + 1 < n1 // 2:
                    send_first(w, colour, k + 1)
                send_second(w, colour, k + 1, 0)
        for step in range(max(Y, Z) // 2):
            for colour in range(2):
                n1, n2 = rings(colour)[0][1], rings(colour)[1][1]
                g = k - step
                if 0 <= g <= n1 // 2 and step < n2 // 2:
                    await_pieces(w, second_count(colour, g, step), recv_sem(w, colour, g, step))
                    if step + 1 < n2 // 2:
                        send_second(w, colour, g, step + 1)

    ticks = (Y + Z) // 2

    def late_tick(k):
        with jax.named_scope(f"late#k={k}"):
            if k < ticks:
                tick(1, k)

    begin(0)
    mine = tokw.at[:, span(tp * dl, dl)]
    for d in range(1, TP):
        remote(mine, mine, tok_sem.at[0], tok_sem.at[1], (fs, (tp + d) % TP)).start()
    mine = gainw.at[:, span(tp * dl, dl)]
    for d in range(1, TP):
        remote(mine, mine, gain_sem.at[0], gain_sem.at[1], (fs, (tp + d) % TP)).start()
    for k in range(ticks):
        with jax.named_scope(f"early#k={k}"):
            tick(0, k)
            if k == ticks - 1 - LATE:
                begin(1)
            if k >= ticks - LATE:
                tick(1, k - (ticks - LATE))
    with jax.named_scope("tokens"):
        await_recv(tokw.at[:, pl.ds(0, (TP - 1) * dl)], tok_sem.at[1])
        await_recv(gainw.at[:, pl.ds(0, (TP - 1) * dl)], gain_sem.at[1])

    def taps_of(v, tap_ref, cols):
        at = lax.broadcasted_iota(jnp.int32, v.shape, 0)
        one = jnp.where(at >= 1, pltpu.roll(v, 1, 0), 0.0)
        two = jnp.where(at >= 2, pltpu.roll(v, 2, 0), 0.0)
        return v * tap_ref[2:3, cols] + one * tap_ref[1:2, cols] + two * tap_ref[0:1, cols]

    def seq(s):
        return pl.ds(s * SEQ_LEN, SEQ_LEN)

    def project(left, g, r, target):
        def one(n, carry):
            at = pl.multiple_of(n * 256, 256)
            right = g[:, :, :, :, pl.ds(at, 256)].reshape(D, 256)
            target[r, pl.ds(at, 256)] = jnp.dot(left[r, :], right, preferred_element_type=F32).astype(BF16)
            return carry

        lax.fori_loop(0, target.shape[1] // 256, one, 0)

    def branch_out(slot, s, left, g, first_col, cols, ppart, pown, dbuf):
        def theirs(j, carry):
            right = g[2 * j + 1 - c, :, :, :, first_col : first_col + cols].reshape(dl, cols)
            ppart[s, j] = nt_dot(left[seq(s), :], right).astype(BF16)
            return carry

        lax.fori_loop(0, X, theirs, 0)
        remote(ppart.at[s], dbuf.at[s], dsend.at[slot], drecv.at[slot * n_seq + s], (fs, partner)).start()

        def ours(j, carry):
            right = g[2 * j + c, :, :, :, first_col : first_col + cols].reshape(dl, cols)
            pown[s, j] = nt_dot(left[seq(s), :], right).astype(BF16)
            return carry

        lax.fori_loop(0, X, ours, 0)

    def cross(slot, s, pown, dbuf, sbuf, rbuf):
        await_recv(dbuf.at[s], drecv.at[slot * n_seq + s])
        for d in away:
            j = (x + d) % X
            sbuf[s, d - 1] = (pown[s, j].astype(F32) + dbuf[s, j].astype(F32)).astype(BF16)
            remote(
                sbuf.at[s, d - 1], rbuf.at[s, d - 1], xsend.at[slot], xrecv.at[slot * n_seq + s], (fs, 2 * j + c)
            ).start()

    def total(slot, s, pown, dbuf, rbuf):
        await_recv(rbuf.at[s], xrecv.at[slot * n_seq + s])
        acc = pown[s, x].astype(F32) + dbuf[s, x].astype(F32)
        for d in away:
            acc = acc + rbuf[s, d - 1].astype(F32)
        return acc

    own_cols = span(tp * dl, dl)

    def mixer(s):
        with jax.named_scope(f"mixer#s={s}"):
            project(tokw, g12, seq(s), proj)
            for at in range(0, dl, 128):
                cols = pl.ds(at, 128)
                outer = proj[seq(s), cols].astype(F32)
                inner = proj[seq(s), pl.ds(dl + at, 128)].astype(F32)
                value = proj[seq(s), pl.ds(2 * dl + at, 128)].astype(F32)
                gated[seq(s), cols] = (outer * taps_of(inner * value, mtapf, cols)).astype(BF16)
            branch_out(0, s, gated, g12, 3 * dl, dl, ppart_m, pown_m, dbuf_m)

    def mixer_cross(s):
        with jax.named_scope(f"mcross#s={s}"):
            cross(0, s, pown_m, dbuf_m, sbuf_m, rbuf_m)

    def gather_start(s):
        with jax.named_scope(f"rs#s={s}"):
            branchw[seq(s), own_cols] = total(0, s, pown_m, dbuf_m, rbuf_m).astype(BF16)
            mine = branchw.at[seq(s), own_cols]
            for d in away:
                remote(mine, mine, agx_send, agx_recv.at[s], (fs, 2 * ((x + d) % X) + c)).start()
            remote(mine, mine, agd_send, agd_recv.at[s], (fs, partner)).start()

    def gather_share(s):
        with jax.named_scope(f"agx#s={s}"):
            await_recv(branchw.at[seq(s), pl.ds(0, (X - 1) * dl)], agx_recv.at[s])
            for d in away:
                theirs = branchw.at[seq(s), span((2 * ((x + d) % X) + c) * dl, dl)]
                remote(theirs, theirs, agd_send, agd_recv.at[s], (fs, partner)).start()

    def first_norm(s):
        with jax.named_scope(f"agd#s={s}"):
            await_recv(branchw.at[seq(s), pl.ds(0, X * dl)], agd_recv.at[s])
        with jax.named_scope(f"norm#s={s}"):
            zero = jnp.zeros((SEQ_LEN, 128), F32)

            def summed(k, acc):
                cols = span(k * 128, 128)
                v = residual_scale * tokw[seq(s), cols].astype(F32) + branchw[seq(s), cols].astype(F32)
                normed[:, cols] = v
                return acc + v

            mean = jnp.sum(lax.fori_loop(0, D // 128, summed, zero), axis=1, keepdims=True) * (1.0 / D)

            def squared(k, acc):
                v = normed[:, span(k * 128, 128)] - mean
                return acc + v * v

            spread = jnp.sum(lax.fori_loop(0, D // 128, squared, zero), axis=1, keepdims=True) * (1.0 / D)
            scale = lax.rsqrt(spread + norm_epsilon)

            def scaled(k, carry):
                cols = span(k * 128, 128)
                firstw[seq(s), cols] = ((normed[:, cols] - mean) * scale * gainw[0:1, cols]).astype(BF16)
                return carry

            lax.fori_loop(0, D // 128, scaled, 0)

    def ffn(s):
        with jax.named_scope(f"ffn#s={s}"):
            project(firstw, g34, seq(s), up)
            for at in range(0, fl, 128):
                cols = pl.ds(at, 128)
                left = taps_of(up[seq(s), cols].astype(F32), gtapf, cols)
                right = taps_of(up[seq(s), pl.ds(fl + at, 128)].astype(F32), vtapf, cols)
                hidden[seq(s), cols] = (left / (1.0 + jnp.exp(-left)) * right).astype(BF16)
            branch_out(1, s, hidden, g34, 2 * fl, fl, ppart_f, pown_f, dbuf_f)

    def ffn_cross(s):
        with jax.named_scope(f"fcross#s={s}"):
            cross(1, s, pown_f, dbuf_f, sbuf_f, rbuf_f)

    lane = lax.broadcasted_iota(jnp.int32, (SEQ_LEN, 128), 1)
    line = lax.broadcasted_iota(jnp.int32, (128, SEQ_LEN), 0)

    def last_sums(s):
        with jax.named_scope(f"frs#s={s}"):
            v = residual_scale * firstw[seq(s), own_cols].astype(F32) + total(1, s, pown_f, dbuf_f, rbuf_f)
            ybuf[seq(s), :] = v
            mean = jnp.sum(v, axis=1, keepdims=True) * (1.0 / dl)
            v = v - mean
            square = jnp.sum(v * v, axis=1, keepdims=True)
            both = jnp.where(lane == 0, mean, jnp.where(lane == 1, square, 0.0))
            stats[tp, s] = both.T[:8]
            for d in range(1, TP):
                remote(stats.at[tp, s], stats.at[tp, s], st_send, st_recv.at[s], (fs, (tp + d) % TP)).start()

    def last_norm(s):
        with jax.named_scope(f"final#s={s}"):
            await_recv(stats.at[pl.ds(0, TP - 1), s], st_recv.at[s])
            theirs = stats[:, s]
            means, squares = theirs[:, 0], theirs[:, 1]
            mean = jnp.sum(means, axis=0, keepdims=True) * (1.0 / TP)
            off = means - mean
            spread = jnp.sum(squares, axis=0, keepdims=True) + dl * jnp.sum(off * off, axis=0, keepdims=True)
            scale = lax.rsqrt(spread * (1.0 / D) + norm_epsilon)
            both = jnp.where(line == 0, mean, jnp.where(line == 1, scale, 0.0)).T
            v = (ybuf[seq(s), :] - both[:, 0:1]) * both[:, 1:2]
            out_ref[seq(s), :] = (v * fgain_ref[...].astype(F32).reshape(1, dl)).astype(BF16)

    plan = [(mixer, s) for s in range(n_seq)]
    for s in range(n_seq):
        plan.insert(2 * s + 2, (mixer_cross, s))
    plan += [(gather_start, s) for s in range(n_seq)]
    for s in range(n_seq):
        plan += [(gather_share, s)] + ([(first_norm, s - 1)] if s > 0 else [])
    plan += [(first_norm, n_seq - 1)]
    late = LATE
    for i, (stage, s) in enumerate(plan):
        if LATE_AT[late] == (stage.__name__, s):
            late_tick(late)
            late += 1
        stage(s)
    while late < ticks:
        late_tick(late)
        late += 1
    plan = [(ffn, s) for s in range(n_seq)]
    for s in range(n_seq):
        plan.insert(2 * s + 2, (ffn_cross, s))
    plan += [(last_sums, s) for s in range(n_seq)] + [(last_norm, s) for s in range(n_seq)]
    for stage, s in plan:
        stage(s)

    with jax.named_scope("drain"):
        for w, g in enumerate(groups):
            await_send(g.at[pl.ds(0, Z - 1), 0], wsend.at[2 * w])
            await_send(g.at[:, pl.ds(0, Y - 1)], wsend.at[2 * w + 1])
        await_send(tokw.at[:, pl.ds(0, (TP - 1) * dl)], tok_sem.at[0])
        await_send(gainw.at[:, pl.ds(0, (TP - 1) * dl)], gain_sem.at[0])
        for slot, (ppart, sbuf) in enumerate(((ppart_m, sbuf_m), (ppart_f, sbuf_f))):
            await_send(ppart, dsend.at[slot])
            await_send(sbuf, xsend.at[slot])
        await_send(branchw.at[:, pl.ds(0, (X - 1) * dl)], agx_send)
        await_send(branchw.at[:, pl.ds(0, X * dl)], agd_send)
        await_send(stats.at[pl.ds(0, TP - 1)], st_send)


def layer(cfg, tokens, outer_gate, inner_gate, mix_value, mix_taps, mix_out, mix_gain, ffn_gate, ffn_value, gate_taps, value_taps, ffn_down, ffn_gain):
    Z, Y, TP = cfg
    X = TP // 2
    rows, dl = tokens.shape
    kr = outer_gate.shape[0]
    h = kr // 2
    fl = ffn_gate.shape[1]
    D = TP * dl
    n_seq = rows // SEQ_LEN
    vmem = pl.BlockSpec(memory_space=pltpu.VMEM)
    hbm = pl.BlockSpec(memory_space=pl.ANY)
    dma = pltpu.SemaphoreType.DMA
    exchange = [
        pltpu.VMEM((n_seq, X, SEQ_LEN, dl), BF16),
        pltpu.VMEM((n_seq, X, SEQ_LEN, dl), BF16),
        pltpu.VMEM((n_seq, X, SEQ_LEN, dl), BF16),
        pltpu.VMEM((n_seq, X - 1, SEQ_LEN, dl), BF16),
        pltpu.VMEM((n_seq, X - 1, SEQ_LEN, dl), BF16),
    ]
    return pl.pallas_call(
        functools.partial(kernel, cfg),
        out_shape=jax.ShapeDtypeStruct((rows, dl), BF16),
        in_specs=[hbm, hbm, hbm, hbm, vmem, hbm, vmem, hbm, hbm, vmem, vmem, hbm, vmem],
        out_specs=vmem,
        scratch_shapes=[
            pltpu.VMEM((Z, Y, 2, h, 4 * dl), BF16),
            pltpu.VMEM((Z, Y, 2, h, 3 * fl), BF16),
            pltpu.VMEM((rows, D), BF16),
            pltpu.VMEM((8, D), F32),
            pltpu.VMEM((rows, D), BF16),
            pltpu.VMEM((rows, D), BF16),
            pltpu.VMEM((SEQ_LEN, D), F32),
            pltpu.VMEM((rows, 3 * dl), BF16),
            pltpu.VMEM((rows, dl), BF16),
            pltpu.VMEM((rows, 2 * fl), BF16),
            pltpu.VMEM((rows, fl), BF16),
            *exchange,
            *exchange,
            pltpu.VMEM((rows, dl), F32),
            pltpu.VMEM((TP, n_seq, 8, SEQ_LEN), F32),
            pltpu.VMEM((3, dl), F32),
            pltpu.VMEM((3, fl), F32),
            pltpu.VMEM((3, fl), F32),
            dma((96,)),
            dma((4,)),
            dma((3,)),
            dma((2,)),
            dma((2,)),
            dma((2,)),
            dma((2 * n_seq,)),
            dma((2,)),
            dma((2 * n_seq,)),
            dma,
            dma((n_seq,)),
            dma,
            dma((n_seq,)),
            dma,
            dma((n_seq,)),
        ],
        compiler_params=pltpu.CompilerParams(
            collective_id=0, has_side_effects=True, vmem_limit_bytes=VMEM_LIMIT
        ),
    )(
        tokens,
        outer_gate,
        inner_gate,
        mix_value,
        mix_taps,
        mix_out.T,
        mix_gain,
        ffn_gate,
        ffn_value,
        gate_taps,
        value_taps,
        ffn_down.T,
        ffn_gain,
    )


def solution(mesh):
    placed = (
        P("fs", "tp"),
        P("fs", "tp"),
        P("fs", "tp"),
        P("fs", "tp"),
        P(None, "tp"),
        P("tp", "fs"),
        P("tp"),
        P("fs", "tp"),
        P("fs", "tp"),
        P(None, "tp"),
        P(None, "tp"),
        P("tp", "fs"),
        P("tp"),
    )
    cfg = (RING_Z, RING_Y, mesh.shape["tp"])
    return jax.shard_map(
        functools.partial(layer, cfg), mesh=mesh, in_specs=placed, out_specs=P("fs", "tp"), check_vma=False
    )
```

```python
import functools

import jax
import jax.numpy as jnp
from jax import lax
from jax.experimental import pallas as pl
from jax.experimental.pallas import tpu as pltpu
from jax.sharding import PartitionSpec as P

SEQ_LEN = 128
RING_Z = 8
RING_Y = 8
residual_scale = 8.0**0.25
norm_epsilon = 1e-05
MESH = pl.DeviceIdType.MESH
RIGHT, LEFT = 0, 1
W34_FIRST = 0
W34_SECOND = (5, 5, 6, 6, 6)
LATE_AT = {
    1: ("mixer_cross", 2),
    2: ("gather_start", 1),
    3: ("gather_share", 0),
    4: ("gather_share", 1),
}
VMEM_LIMIT = 60 * 1024 * 1024
F32 = jnp.float32
BF16 = jnp.bfloat16


def kernel(
    cfg,
    tok_ref,
    og_ref,
    ig_ref,
    mv_ref,
    mtaps_ref,
    mo_ref,
    mgain_ref,
    fg_ref,
    fv_ref,
    gtaps_ref,
    vtaps_ref,
    fd_ref,
    fgain_ref,
    out_ref,
    g12,
    g34,
    tokw,
    gainw,
    branchw,
    firstw,
    normed,
    psum,
    proj,
    gated,
    up,
    hidden,
    ppart_m,
    pown_m,
    dbuf_m,
    sbuf_m,
    rbuf_m,
    ppart_f,
    pown_f,
    dbuf_f,
    sbuf_f,
    rbuf_f,
    ybuf,
    stats,
    mtapf,
    gtapf,
    vtapf,
    wrecv,
    wsend,
    loc_sem,
    tok_sem,
    gain_sem,
    dsend,
    drecv,
    xsend,
    xrecv,
    agx_send,
    agx_recv,
    agd_send,
    agd_recv,
    st_send,
    st_recv,
):
    Z, Y, TP = cfg
    X = TP // 2
    rows, dl = tok_ref.shape
    kr = og_ref.shape[0]
    h = kr // 2
    fl = fg_ref.shape[1]
    D = TP * dl
    n_seq = rows // SEQ_LEN
    fs = lax.axis_index("fs")
    tp = lax.axis_index("tp")
    z, y = fs // Y, fs % Y
    x, c = tp // 2, tp % 2
    partner = 2 * x + (1 - c)
    groups = (g12, g34)
    away = list(dict.fromkeys([X // 2, *range(1, X)]))

    def ring_id(axis, step):
        if axis == "y":
            return (z * Y + (y + step + Y) % Y, tp)
        return (((z + step + Z) % Z) * Y + y, tp)

    def span(at, size):
        return pl.ds(pl.multiple_of(at, size), size)

    def remote(src, dst, send_sem, recv_sem, to):
        return pltpu.make_async_remote_copy(
            src_ref=src, dst_ref=dst, send_sem=send_sem, recv_sem=recv_sem, device_id=to, device_id_type=MESH
        )

    def await_recv(box, sem):
        remote(box, box, sem, sem, (fs, partner)).wait_recv()

    def await_send(box, sem):
        remote(box, box, sem, sem, (fs, partner)).wait_send()

    barrier = pltpu.get_barrier_semaphore()
    for axis in ("y", "z"):
        for step in (1, -1, 2, -2):
            pl.semaphore_signal(barrier, inc=1, device_id=ring_id(axis, step), device_id_type=MESH)
    for d in range(1, TP):
        pl.semaphore_signal(barrier, inc=1, device_id=(fs, (tp + d) % TP), device_id_type=MESH)

    def place(g, refs, sem):
        at = 0
        for ref in refs:
            cols = ref.shape[1]
            for half in range(2):
                pltpu.make_async_copy(
                    ref.at[pl.ds(half * h, h)], g.at[z, y, half, :, pl.ds(at, cols)], sem
                ).start()
            at += cols

    own_tokens = pltpu.make_async_copy(tok_ref, tokw.at[:, span(tp * dl, dl)], loc_sem.at[2])
    place(g12, (og_ref, ig_ref, mv_ref, mo_ref), loc_sem.at[0])
    own_tokens.start()
    place(g34, (fg_ref, fv_ref, fd_ref), loc_sem.at[1])
    gainw[:, span(tp * dl, dl)] = jnp.broadcast_to(mgain_ref[...].astype(F32).reshape(1, dl), (8, dl))
    mtapf[...] = mtaps_ref[...].astype(F32)
    gtapf[...] = gtaps_ref[...].astype(F32)
    vtapf[...] = vtaps_ref[...].astype(F32)
    for i, g in enumerate(groups):
        pltpu.make_async_copy(g.at[z, y], g.at[z, y], loc_sem.at[i]).wait()
    own_tokens.wait()
    with jax.named_scope("greet"):
        pl.semaphore_wait(barrier, 8 + TP - 1)

    def piece(w, colour, one, two):
        return groups[w].at[two, one, 0] if colour == 0 else groups[w].at[one, two, 1]

    def rings(colour):
        return (("y", Y, y), ("z", Z, z)) if colour == 0 else (("z", Z, z), ("y", Y, y))

    def recv_sem(w, colour, kind, step):
        return wrecv.at[((w * 2 + colour) * 6 + kind) * 4 + step]

    def send_first(w, colour, step):
        (axis, n, me), (_, _, other) = rings(colour)
        for way in (RIGHT, LEFT):
            if step == n // 2 - 1 and way != w % 2:
                continue
            straight = w == 0 and step == 1 and n >= 8
            reach, back = (2, 0) if straight else (1, step)
            origin = (me - back + n) % n if way == RIGHT else (me + back) % n
            ref = piece(w, colour, origin, other)
            remote(
                ref, ref, wsend.at[2 * w], recv_sem(w, colour, 5, step), ring_id(axis, reach if way == RIGHT else -reach)
            ).start()

    def first_count(colour, step):
        return 1 if step == rings(colour)[0][1] // 2 - 1 else 2

    def members(n, g):
        return [0] if g == 0 else [g] if g == n // 2 else [g, -g]

    def halves(n, g):
        return ([0], []) if g == 0 else ([], [g]) if g == n // 2 else ([g], [-g])

    def send_second(w, colour, g, step):
        (_, n1, me1), (axis, n2, me2) = rings(colour)
        for way in (RIGHT, LEFT):
            at = members(n1, g) if step < n2 // 2 - 1 else halves(n1, g)[way]
            origin = (me2 - step + n2) % n2 if way == RIGHT else (me2 + step) % n2
            for m in at:
                ref = piece(w, colour, (me1 + m + n1) % n1, origin)
                remote(
                    ref, ref, wsend.at[2 * w + 1], recv_sem(w, colour, g, step), ring_id(axis, 1 if way == RIGHT else -1)
                ).start()

    def second_count(colour, g, step):
        n1, n2 = rings(colour)[0][1], rings(colour)[1][1]
        if step < n2 // 2 - 1:
            return 2 * len(members(n1, g))
        return sum(len(part) for part in halves(n1, g))

    def await_pieces(w, count, sem):
        g = groups[w]
        await_recv(g.at[0, 0, 0] if count == 1 else g.at[pl.ds(0, count), 0, 0], sem)

    def first_arrives(w, k):
        for colour in range(2):
            n1 = rings(colour)[0][1]
            if k < n1 // 2:
                await_pieces(w, first_count(colour, k), recv_sem(w, colour, 5, k))
                if k + 1 < n1 // 2 and (w == 1 or k > 0 or n1 < 8):
                    send_first(w, colour, k + 1)

    def second_begins(w, g):
        for colour in range(2):
            if g <= rings(colour)[0][1] // 2:
                send_second(w, colour, g, 0)

    def second_arrives(w, g, step):
        for colour in range(2):
            n1, n2 = rings(colour)[0][1], rings(colour)[1][1]
            if g <= n1 // 2 and step < n2 // 2:
                await_pieces(w, second_count(colour, g, step), recv_sem(w, colour, g, step))
                if step + 1 < n2 // 2:
                    send_second(w, colour, g, step + 1)

    most = max(Y, Z) // 2
    first_tick = {(0, k): max(0, k - 1) if most >= 4 else k for k in range(most)}
    first_tick.update({(1, k): W34_FIRST + 1 + k for k in range(most)})
    second_tick = {(0, g): first_tick[0, g - 1] if g > 0 else -1 for g in range(most + 1)}
    for g in range(most + 1):
        second_tick[1, g] = max(W34_SECOND[min(g, 4)], first_tick[1, g - 1] if g > 0 else 0)
    ready = max(second_tick[0, g] for g in range(most + 1)) + most
    ticks = max(second_tick[1, g] for g in range(most + 1)) + most

    def tick(at):
        for w in range(2):
            firsts = [k for k in range(most) if first_tick[w, k] == at]
            for k in firsts[:1]:
                first_arrives(w, k)
                if w == 0:
                    second_begins(w, k + 1)
            for step in range(most):
                for g in range(most + 1):
                    if second_tick[w, g] + 1 + step == at:
                        second_arrives(w, g, step)
            for k in firsts[1:]:
                first_arrives(w, k)
                if w == 0:
                    second_begins(w, k + 1)
            if w == 1:
                if at == W34_FIRST:
                    for colour in range(2):
                        send_first(1, colour, 0)
                for g in range(most + 1):
                    if second_tick[1, g] == at:
                        second_begins(1, g)

    def late_tick(k):
        with jax.named_scope(f"late#k={k}"):
            tick(k)

    for colour in range(2):
        send_first(0, colour, 0)
    second_begins(0, 0)
    for colour in range(2):
        if rings(colour)[0][1] >= 8:
            send_first(0, colour, 1)
    mine = tokw.at[:, span(tp * dl, dl)]
    for d in range(1, TP):
        remote(mine, mine, tok_sem.at[0], tok_sem.at[1], (fs, (tp + d) % TP)).start()
    mine = gainw.at[:, span(tp * dl, dl)]
    for d in range(1, TP):
        remote(mine, mine, gain_sem.at[0], gain_sem.at[1], (fs, (tp + d) % TP)).start()
    for k in range(ready):
        with jax.named_scope(f"early#k={k}"):
            tick(k)
    with jax.named_scope("tokens"):
        await_recv(tokw.at[:, pl.ds(0, (TP - 1) * dl)], tok_sem.at[1])
        await_recv(gainw.at[:, pl.ds(0, (TP - 1) * dl)], gain_sem.at[1])

    deep = D // Z

    def plane_dot(plane, at):
        right = g12[plane, :, :, :, pl.ds(at, 256)].reshape(deep, 256)
        return jnp.dot(tokw[:, span(plane * deep, deep)], right, preferred_element_type=F32)

    with jax.named_scope("planes"):
        for at in range(0, 3 * dl, 256):
            psum[:, at : at + 256] = plane_dot((z + Z // 2 + 1) % Z, at)

        def add_plane(i, carry):
            for at in range(0, 3 * dl, 256):
                psum[:, at : at + 256] += plane_dot((z + Z // 2 + i) % Z, at)
            return carry

        lax.fori_loop(2, Z, add_plane, 0)
    with jax.named_scope(f"early#k={ready}"):
        tick(ready)

    def taps_of(v, tap_ref, cols):
        at = lax.broadcasted_iota(jnp.int32, v.shape, 0)
        one = jnp.where(at >= 1, pltpu.roll(v, 1, 0), 0.0)
        two = jnp.where(at >= 2, pltpu.roll(v, 2, 0), 0.0)
        return v * tap_ref[2:3, cols] + one * tap_ref[1:2, cols] + two * tap_ref[0:1, cols]

    def seq(s):
        return pl.ds(s * SEQ_LEN, SEQ_LEN)

    def project(left, g, r, target):
        def one(n, carry):
            at = pl.multiple_of(n * 256, 256)
            right = g[:, :, :, :, pl.ds(at, 256)].reshape(D, 256)
            target[r, pl.ds(at, 256)] = jnp.dot(left[r, :], right, preferred_element_type=F32).astype(BF16)
            return carry

        lax.fori_loop(0, target.shape[1] // 256, one, 0)

    def branch_out(slot, s, turned, g, first_col, cols, ppart, pown, dbuf):
        def theirs(j, carry):
            left = g[2 * j + 1 - c, :, :, :, first_col : first_col + cols].reshape(dl, cols)
            ppart[s, j] = jnp.dot(left, turned[s], preferred_element_type=F32).astype(BF16)
            return carry

        lax.fori_loop(0, X, theirs, 0, unroll=True)
        remote(ppart.at[s], dbuf.at[s], dsend.at[slot], drecv.at[slot * n_seq + s], (fs, partner)).start()

        def ours(j, carry):
            left = g[2 * j + c, :, :, :, first_col : first_col + cols].reshape(dl, cols)
            pown[s, j] = jnp.dot(left, turned[s], preferred_element_type=F32).astype(BF16)
            return carry

        lax.fori_loop(0, X, ours, 0, unroll=True)

    def cross(slot, s, pown, dbuf, sbuf, rbuf):
        await_recv(dbuf.at[s], drecv.at[slot * n_seq + s])
        for d in away:
            j = (x + d) % X
            sbuf[s, d - 1] = (pown[s, j].astype(F32) + dbuf[s, j].astype(F32)).astype(BF16)
            remote(
                sbuf.at[s, d - 1], rbuf.at[s, d - 1], xsend.at[slot], xrecv.at[slot * n_seq + s], (fs, 2 * j + c)
            ).start()

    def total(slot, s, pown, dbuf, rbuf):
        await_recv(rbuf.at[s], xrecv.at[slot * n_seq + s])
        acc = pown[s, x].astype(F32) + dbuf[s, x].astype(F32)
        for d in away:
            acc = acc + rbuf[s, d - 1].astype(F32)
        return acc.T

    own_cols = span(tp * dl, dl)

    def mixer(s):
        with jax.named_scope(f"mixer#s={s}"):
            if s == 0:
                for at in range(0, 3 * dl, 256):
                    last = psum[:, at : at + 256] + plane_dot((z + Z // 2) % Z, at)
                    proj[:, at : at + 256] = last.astype(BF16)
            for at in range(0, dl, 128):
                cols = pl.ds(at, 128)
                outer = proj[seq(s), cols].astype(F32)
                inner = proj[seq(s), pl.ds(dl + at, 128)].astype(F32)
                value = proj[seq(s), pl.ds(2 * dl + at, 128)].astype(F32)
                gated[s, cols, :] = (outer * taps_of(inner * value, mtapf, cols)).T.astype(BF16)
            branch_out(0, s, gated, g12, 3 * dl, dl, ppart_m, pown_m, dbuf_m)

    def mixer_cross(s):
        with jax.named_scope(f"mcross#s={s}"):
            cross(0, s, pown_m, dbuf_m, sbuf_m, rbuf_m)

    def gather_start(s):
        with jax.named_scope(f"rs#s={s}"):
            branchw[seq(s), own_cols] = total(0, s, pown_m, dbuf_m, rbuf_m).astype(BF16)
            mine = branchw.at[seq(s), own_cols]
            for d in away:
                remote(mine, mine, agx_send, agx_recv.at[s], (fs, 2 * ((x + d) % X) + c)).start()
            remote(mine, mine, agd_send, agd_recv.at[s], (fs, partner)).start()

    def gather_share(s):
        with jax.named_scope(f"agx#s={s}"):
            await_recv(branchw.at[seq(s), pl.ds(0, (X - 1) * dl)], agx_recv.at[s])
            for d in away:
                theirs = branchw.at[seq(s), span((2 * ((x + d) % X) + c) * dl, dl)]
                remote(theirs, theirs, agd_send, agd_recv.at[s], (fs, partner)).start()

    def first_norm(s):
        with jax.named_scope(f"agd#s={s}"):
            await_recv(branchw.at[seq(s), pl.ds(0, X * dl)], agd_recv.at[s])
        with jax.named_scope(f"norm#s={s}"):
            zero = jnp.zeros((SEQ_LEN, 128), F32)

            def summed(k, acc):
                cols = span(k * 128, 128)
                v = residual_scale * tokw[seq(s), cols].astype(F32) + branchw[seq(s), cols].astype(F32)
                normed[:, cols] = v
                return acc + v

            mean = jnp.sum(lax.fori_loop(0, D // 128, summed, zero, unroll=4), axis=1, keepdims=True) * (1.0 / D)

            def squared(k, acc):
                v = normed[:, span(k * 128, 128)] - mean
                return acc + v * v

            spread = jnp.sum(lax.fori_loop(0, D // 128, squared, zero, unroll=4), axis=1, keepdims=True) * (1.0 / D)
            scale = lax.rsqrt(spread + norm_epsilon)

            def scaled(k, carry):
                cols = span(k * 128, 128)
                firstw[seq(s), cols] = ((normed[:, cols] - mean) * scale * gainw[0:1, cols]).astype(BF16)
                return carry

            lax.fori_loop(0, D // 128, scaled, 0, unroll=4)

    def ffn(s):
        with jax.named_scope(f"ffn#s={s}"):
            project(firstw, g34, seq(s), up)
            for at in range(0, fl, 128):
                cols = pl.ds(at, 128)
                left = taps_of(up[seq(s), cols].astype(F32), gtapf, cols)
                right = taps_of(up[seq(s), pl.ds(fl + at, 128)].astype(F32), vtapf, cols)
                hidden[s, cols, :] = (left / (1.0 + jnp.exp(-left)) * right).T.astype(BF16)
            branch_out(1, s, hidden, g34, 2 * fl, fl, ppart_f, pown_f, dbuf_f)

    def ffn_cross(s):
        with jax.named_scope(f"fcross#s={s}"):
            cross(1, s, pown_f, dbuf_f, sbuf_f, rbuf_f)

    lane = lax.broadcasted_iota(jnp.int32, (SEQ_LEN, 128), 1)
    line = lax.broadcasted_iota(jnp.int32, (128, SEQ_LEN), 0)

    def last_sums(s):
        with jax.named_scope(f"frs#s={s}"):
            v = residual_scale * firstw[seq(s), own_cols].astype(F32) + total(1, s, pown_f, dbuf_f, rbuf_f)
            ybuf[seq(s), :] = v
            mean = jnp.sum(v, axis=1, keepdims=True) * (1.0 / dl)
            v = v - mean
            square = jnp.sum(v * v, axis=1, keepdims=True)
            both = jnp.where(lane == 0, mean, jnp.where(lane == 1, square, 0.0))
            stats[tp, s] = both.T[:8]
            for d in range(1, TP):
                remote(stats.at[tp, s], stats.at[tp, s], st_send, st_recv.at[s], (fs, (tp + d) % TP)).start()

    def last_norm(s):
        with jax.named_scope(f"final#s={s}"):
            await_recv(stats.at[pl.ds(0, TP - 1), s], st_recv.at[s])
            theirs = stats[:, s]
            means, squares = theirs[:, 0], theirs[:, 1]
            mean = jnp.sum(means, axis=0, keepdims=True) * (1.0 / TP)
            off = means - mean
            spread = jnp.sum(squares, axis=0, keepdims=True) + dl * jnp.sum(off * off, axis=0, keepdims=True)
            scale = lax.rsqrt(spread * (1.0 / D) + norm_epsilon)
            both = jnp.where(line == 0, mean, jnp.where(line == 1, scale, 0.0)).T
            v = (ybuf[seq(s), :] - both[:, 0:1]) * both[:, 1:2]
            out_ref[seq(s), :] = (v * fgain_ref[...].astype(F32).reshape(1, dl)).astype(BF16)

    plan = [(mixer, s) for s in range(n_seq)]
    for s in range(n_seq):
        plan.insert(2 * s + 2, (mixer_cross, s))
    plan += [(gather_start, s) for s in range(n_seq)] + [(gather_share, s) for s in range(n_seq)]
    for s in range(n_seq):
        plan += [(first_norm, s)] + ([(ffn_cross, s - 1)] if s > 0 else []) + [(ffn, s)]
    plan += [(ffn_cross, n_seq - 1)]
    share = plan.index((gather_share, n_seq - 1))
    plan.insert(min(share + 2, len(plan)), plan.pop(share))
    late = ready + 1
    plan += [(last_sums, s) for s in range(n_seq)] + [(last_norm, s) for s in range(n_seq)]
    for stage, s in plan:
        while late <= ticks and (LATE_AT.get(late - ready) == (stage.__name__, s) or stage is first_norm):
            late_tick(late)
            late += 1
        stage(s)

    with jax.named_scope("drain"):
        for w, g in enumerate(groups):
            await_send(g.at[pl.ds(0, Z - 1), 0], wsend.at[2 * w])
            await_send(g.at[:, pl.ds(0, Y - 1)], wsend.at[2 * w + 1])
        await_send(tokw.at[:, pl.ds(0, (TP - 1) * dl)], tok_sem.at[0])
        await_send(gainw.at[:, pl.ds(0, (TP - 1) * dl)], gain_sem.at[0])
        for slot, (ppart, sbuf) in enumerate(((ppart_m, sbuf_m), (ppart_f, sbuf_f))):
            await_send(ppart, dsend.at[slot])
            await_send(sbuf, xsend.at[slot])
        await_send(branchw.at[:, pl.ds(0, (X - 1) * dl)], agx_send)
        await_send(branchw.at[:, pl.ds(0, X * dl)], agd_send)
        await_send(stats.at[pl.ds(0, TP - 1)], st_send)


def layer(cfg, tokens, outer_gate, inner_gate, mix_value, mix_taps, mix_out, mix_gain, ffn_gate, ffn_value, gate_taps, value_taps, ffn_down, ffn_gain):
    Z, Y, TP = cfg
    X = TP // 2
    rows, dl = tokens.shape
    kr = outer_gate.shape[0]
    h = kr // 2
    fl = ffn_gate.shape[1]
    D = TP * dl
    n_seq = rows // SEQ_LEN
    vmem = pl.BlockSpec(memory_space=pltpu.VMEM)
    hbm = pl.BlockSpec(memory_space=pl.ANY)
    dma = pltpu.SemaphoreType.DMA
    exchange = [
        pltpu.VMEM((n_seq, X, dl, SEQ_LEN), BF16),
        pltpu.VMEM((n_seq, X, dl, SEQ_LEN), BF16),
        pltpu.VMEM((n_seq, X, dl, SEQ_LEN), BF16),
        pltpu.VMEM((n_seq, X - 1, dl, SEQ_LEN), BF16),
        pltpu.VMEM((n_seq, X - 1, dl, SEQ_LEN), BF16),
    ]
    return pl.pallas_call(
        functools.partial(kernel, cfg),
        out_shape=jax.ShapeDtypeStruct((rows, dl), BF16),
        in_specs=[hbm, hbm, hbm, hbm, vmem, hbm, vmem, hbm, hbm, vmem, vmem, hbm, vmem],
        out_specs=vmem,
        scratch_shapes=[
            pltpu.VMEM((Z, Y, 2, h, 4 * dl), BF16),
            pltpu.VMEM((Z, Y, 2, h, 3 * fl), BF16),
            pltpu.VMEM((rows, D), BF16),
            pltpu.VMEM((8, D), F32),
            pltpu.VMEM((rows, D), BF16),
            pltpu.VMEM((rows, D), BF16),
            pltpu.VMEM((SEQ_LEN, D), F32),
            pltpu.VMEM((rows, 3 * dl), F32),
            pltpu.VMEM((rows, 3 * dl), BF16),
            pltpu.VMEM((n_seq, dl, SEQ_LEN), BF16),
            pltpu.VMEM((rows, 2 * fl), BF16),
            pltpu.VMEM((n_seq, fl, SEQ_LEN), BF16),
            *exchange,
            *exchange,
            pltpu.VMEM((rows, dl), F32),
            pltpu.VMEM((TP, n_seq, 8, SEQ_LEN), F32),
            pltpu.VMEM((3, dl), F32),
            pltpu.VMEM((3, fl), F32),
            pltpu.VMEM((3, fl), F32),
            dma((96,)),
            dma((4,)),
            dma((3,)),
            dma((2,)),
            dma((2,)),
            dma((2,)),
            dma((2 * n_seq,)),
            dma((2,)),
            dma((2 * n_seq,)),
            dma,
            dma((n_seq,)),
            dma,
            dma((n_seq,)),
            dma,
            dma((n_seq,)),
        ],
        compiler_params=pltpu.CompilerParams(
            collective_id=0, has_side_effects=True, vmem_limit_bytes=VMEM_LIMIT
        ),
    )(
        tokens,
        outer_gate,
        inner_gate,
        mix_value,
        mix_taps,
        mix_out.T,
        mix_gain,
        ffn_gate,
        ffn_value,
        gate_taps,
        value_taps,
        ffn_down.T,
        ffn_gain,
    )


def solution(mesh):
    placed = (
        P("fs", "tp"),
        P("fs", "tp"),
        P("fs", "tp"),
        P("fs", "tp"),
        P(None, "tp"),
        P("tp", "fs"),
        P("tp"),
        P("fs", "tp"),
        P("fs", "tp"),
        P(None, "tp"),
        P(None, "tp"),
        P("tp", "fs"),
        P("tp"),
    )
    cfg = (RING_Z, RING_Y, mesh.shape["tp"])
    return jax.shard_map(
        functools.partial(layer, cfg), mesh=mesh, in_specs=placed, out_specs=P("fs", "tp"), check_vma=False
    )
```

```python
import functools

import jax
import jax.numpy as jnp
from jax import lax
from jax.experimental import pallas as pl
from jax.experimental.pallas import tpu as pltpu
from jax.sharding import PartitionSpec as P

SEQ_LEN = 128
RING_Z = 8
RING_Y = 8
residual_scale = 8.0**0.25
norm_epsilon = 1e-05
MESH = pl.DeviceIdType.MESH
RIGHT, LEFT = 0, 1
W34_FIRST = 0
W34_SECOND = (6, 6, 6, 6, 6)
LATE_AT = {
    1: ("gather_start", 0),
    2: ("gather_start", 1),
    3: ("gather_share", 0),
    4: ("gather_share", 1),
}
VMEM_LIMIT = 60 * 1024 * 1024
F32 = jnp.float32
BF16 = jnp.bfloat16


def kernel(
    cfg,
    tok_ref,
    og_ref,
    ig_ref,
    mv_ref,
    mtaps_ref,
    mo_ref,
    mgain_ref,
    fg_ref,
    fv_ref,
    gtaps_ref,
    vtaps_ref,
    fd_ref,
    fgain_ref,
    out_ref,
    g12,
    g34,
    tokw,
    gainw,
    branchw,
    firstw,
    normed,
    psum,
    proj,
    gated,
    up,
    hidden,
    ppart_m,
    pown_m,
    dbuf_m,
    sbuf_m,
    rbuf_m,
    ppart_f,
    pown_f,
    dbuf_f,
    sbuf_f,
    rbuf_f,
    ybuf,
    stats,
    mtapf,
    gtapf,
    vtapf,
    wrecv,
    wsend,
    loc_sem,
    tok_sem,
    gain_sem,
    dsend,
    drecv,
    xsend,
    xrecv,
    agx_send,
    agx_recv,
    agd_send,
    agd_recv,
    st_send,
    st_recv,
):
    Z, Y, TP = cfg
    X = TP // 2
    rows, dl = tok_ref.shape
    kr = og_ref.shape[0]
    h = kr // 2
    fl = fg_ref.shape[1]
    D = TP * dl
    n_seq = rows // SEQ_LEN
    fs = lax.axis_index("fs")
    tp = lax.axis_index("tp")
    z, y = fs // Y, fs % Y
    x, c = tp // 2, tp % 2
    partner = 2 * x + (1 - c)
    groups = (g12, g34)
    away = list(dict.fromkeys([X // 2, *range(1, X)]))

    def ring_id(axis, step):
        if axis == "y":
            return (z * Y + (y + step + Y) % Y, tp)
        return (((z + step + Z) % Z) * Y + y, tp)

    def span(at, size):
        return pl.ds(pl.multiple_of(at, size), size)

    def remote(src, dst, send_sem, recv_sem, to):
        return pltpu.make_async_remote_copy(
            src_ref=src, dst_ref=dst, send_sem=send_sem, recv_sem=recv_sem, device_id=to, device_id_type=MESH
        )

    def await_recv(box, sem):
        remote(box, box, sem, sem, (fs, partner)).wait_recv()

    def await_send(box, sem):
        remote(box, box, sem, sem, (fs, partner)).wait_send()

    barrier = pltpu.get_barrier_semaphore()
    for axis in ("y", "z"):
        for step in (1, -1, 2, -2):
            pl.semaphore_signal(barrier, inc=1, device_id=ring_id(axis, step), device_id_type=MESH)
    for d in range(1, TP):
        pl.semaphore_signal(barrier, inc=1, device_id=(fs, (tp + d) % TP), device_id_type=MESH)

    def place(g, refs, sem):
        at = 0
        for ref in refs:
            cols = ref.shape[1]
            for half in range(2):
                pltpu.make_async_copy(
                    ref.at[pl.ds(half * h, h)], g.at[z, y, half, :, pl.ds(at, cols)], sem
                ).start()
            at += cols

    own_tokens = pltpu.make_async_copy(tok_ref, tokw.at[:, span(tp * dl, dl)], loc_sem.at[2])
    place(g12, (og_ref, ig_ref, mv_ref, mo_ref), loc_sem.at[0])
    own_tokens.start()
    place(g34, (fg_ref, fv_ref, fd_ref), loc_sem.at[1])
    gainw[:, span(tp * dl, dl)] = jnp.broadcast_to(mgain_ref[...].astype(F32).reshape(1, dl), (8, dl))
    mtapf[...] = mtaps_ref[...].astype(F32)
    gtapf[...] = gtaps_ref[...].astype(F32)
    vtapf[...] = vtaps_ref[...].astype(F32)

    def placed(w):
        pltpu.make_async_copy(groups[w].at[z, y], groups[w].at[z, y], loc_sem.at[w]).wait()

    placed(0)
    with jax.named_scope("greet"):
        pl.semaphore_wait(barrier, 8 + TP - 1)

    def piece(w, colour, one, two):
        return groups[w].at[two, one, 0] if colour == 0 else groups[w].at[one, two, 1]

    def rings(colour):
        return (("y", Y, y), ("z", Z, z)) if colour == 0 else (("z", Z, z), ("y", Y, y))

    def recv_sem(w, colour, kind, step):
        return wrecv.at[((w * 2 + colour) * 6 + kind) * 4 + step]

    def send_first(w, colour, step):
        (axis, n, me), (_, _, other) = rings(colour)
        for way in (RIGHT, LEFT):
            if step == n // 2 - 1 and way != w % 2:
                continue
            straight = w == 0 and step == 1 and n >= 8
            reach, back = (2, 0) if straight else (1, step)
            origin = (me - back + n) % n if way == RIGHT else (me + back) % n
            ref = piece(w, colour, origin, other)
            remote(
                ref, ref, wsend.at[2 * w], recv_sem(w, colour, 5, step), ring_id(axis, reach if way == RIGHT else -reach)
            ).start()

    def first_count(colour, step):
        return 1 if step == rings(colour)[0][1] // 2 - 1 else 2

    def members(n, g):
        return [0] if g == 0 else [g] if g == n // 2 else [g, -g]

    def halves(n, g):
        return ([0], []) if g == 0 else ([], [g]) if g == n // 2 else ([g], [-g])

    def send_second(w, colour, g, step):
        (_, n1, me1), (axis, n2, me2) = rings(colour)
        for way in (RIGHT, LEFT):
            at = members(n1, g) if step < n2 // 2 - 1 else halves(n1, g)[way]
            origin = (me2 - step + n2) % n2 if way == RIGHT else (me2 + step) % n2
            for m in at:
                ref = piece(w, colour, (me1 + m + n1) % n1, origin)
                remote(
                    ref, ref, wsend.at[2 * w + 1], recv_sem(w, colour, g, step), ring_id(axis, 1 if way == RIGHT else -1)
                ).start()

    def second_count(colour, g, step):
        n1, n2 = rings(colour)[0][1], rings(colour)[1][1]
        if step < n2 // 2 - 1:
            return 2 * len(members(n1, g))
        return sum(len(part) for part in halves(n1, g))

    def await_pieces(w, count, sem):
        g = groups[w]
        await_recv(g.at[0, 0, 0] if count == 1 else g.at[pl.ds(0, count), 0, 0], sem)

    def first_arrives(w, k):
        for colour in range(2):
            n1 = rings(colour)[0][1]
            if k < n1 // 2:
                await_pieces(w, first_count(colour, k), recv_sem(w, colour, 5, k))
                if k + 1 < n1 // 2 and (w == 1 or k > 0 or n1 < 8):
                    send_first(w, colour, k + 1)

    def second_begins(w, g):
        for colour in range(2):
            if g <= rings(colour)[0][1] // 2:
                send_second(w, colour, g, 0)

    def second_arrives(w, g, step):
        for colour in range(2):
            n1, n2 = rings(colour)[0][1], rings(colour)[1][1]
            if g <= n1 // 2 and step < n2 // 2:
                await_pieces(w, second_count(colour, g, step), recv_sem(w, colour, g, step))
                if step + 1 < n2 // 2:
                    send_second(w, colour, g, step + 1)

    most = max(Y, Z) // 2
    first_tick = {(0, k): max(0, k - 1) if most >= 4 else k for k in range(most)}
    first_tick.update({(1, k): W34_FIRST + 1 + k for k in range(most)})
    second_tick = {(0, g): first_tick[0, g - 1] if g > 0 else -1 for g in range(most + 1)}
    for g in range(most + 1):
        second_tick[1, g] = max(W34_SECOND[min(g, 4)], first_tick[1, g - 1] if g > 0 else 0)
    ready = max(second_tick[0, g] for g in range(most + 1)) + most
    ticks = max(second_tick[1, g] for g in range(most + 1)) + most

    def tick(at):
        for w in range(2):
            firsts = [k for k in range(most) if first_tick[w, k] == at]
            for k in firsts[:1]:
                first_arrives(w, k)
                if w == 0:
                    second_begins(w, k + 1)
            for step in range(most):
                for g in range(most + 1):
                    if second_tick[w, g] + 1 + step == at:
                        second_arrives(w, g, step)
            for k in firsts[1:]:
                first_arrives(w, k)
                if w == 0:
                    second_begins(w, k + 1)
            if w == 1:
                if at == W34_FIRST:
                    placed(1)
                    for colour in range(2):
                        send_first(1, colour, 0)
                for g in range(most + 1):
                    if second_tick[1, g] == at:
                        second_begins(1, g)

    def late_tick(k):
        with jax.named_scope(f"late#k={k}"):
            tick(k)

    for colour in range(2):
        send_first(0, colour, 0)
    second_begins(0, 0)
    for colour in range(2):
        if rings(colour)[0][1] >= 8:
            send_first(0, colour, 1)
    own_tokens.wait()
    mine = tokw.at[:, span(tp * dl, dl)]
    for d in range(1, TP):
        remote(mine, mine, tok_sem.at[0], tok_sem.at[1], (fs, (tp + d) % TP)).start()
    mine = gainw.at[:, span(tp * dl, dl)]
    for d in range(1, TP):
        remote(mine, mine, gain_sem.at[0], gain_sem.at[1], (fs, (tp + d) % TP)).start()
    for k in range(ready):
        with jax.named_scope(f"early#k={k}"):
            tick(k)
    with jax.named_scope("tokens"):
        await_recv(tokw.at[:, pl.ds(0, (TP - 1) * dl)], tok_sem.at[1])
        await_recv(gainw.at[:, pl.ds(0, (TP - 1) * dl)], gain_sem.at[1])

    deep = D // Z

    def plane_dot(plane, at):
        right = g12[plane, :, :, :, pl.ds(at, 256)].reshape(deep, 256)
        return jnp.dot(tokw[:, span(plane * deep, deep)], right, preferred_element_type=F32)

    with jax.named_scope("planes"):
        for at in range(0, 3 * dl, 256):
            psum[:, at : at + 256] = plane_dot((z + Z // 2 + 1) % Z, at)

        def add_plane(i, carry):
            for at in range(0, 3 * dl, 256):
                psum[:, at : at + 256] += plane_dot((z + Z // 2 + i) % Z, at)
            return carry

        lax.fori_loop(2, Z, add_plane, 0)
    with jax.named_scope(f"early#k={ready}"):
        tick(ready)

    def taps_of(v, tap_ref, cols):
        at = lax.broadcasted_iota(jnp.int32, v.shape, 0)
        one = jnp.where(at >= 1, pltpu.roll(v, 1, 0), 0.0)
        two = jnp.where(at >= 2, pltpu.roll(v, 2, 0), 0.0)
        return v * tap_ref[2:3, cols] + one * tap_ref[1:2, cols] + two * tap_ref[0:1, cols]

    def seq(s):
        return pl.ds(s * SEQ_LEN, SEQ_LEN)

    def project(left, g, r, target):
        def one(n, carry):
            at = pl.multiple_of(n * 256, 256)
            right = g[:, :, :, :, pl.ds(at, 256)].reshape(D, 256)
            target[r, pl.ds(at, 256)] = jnp.dot(left[r, :], right, preferred_element_type=F32).astype(BF16)
            return carry

        lax.fori_loop(0, target.shape[1] // 256, one, 0)

    def branch_out(slot, s, turned, g, first_col, cols, ppart, pown, dbuf):
        def theirs(j, carry):
            left = g[2 * j + 1 - c, :, :, :, first_col : first_col + cols].reshape(dl, cols)
            ppart[s, j] = jnp.dot(left, turned[s], preferred_element_type=F32).astype(BF16)
            return carry

        lax.fori_loop(0, X, theirs, 0, unroll=True)
        remote(ppart.at[s], dbuf.at[s], dsend.at[slot], drecv.at[slot * n_seq + s], (fs, partner)).start()

        def ours(j, carry):
            left = g[2 * j + c, :, :, :, first_col : first_col + cols].reshape(dl, cols)
            pown[s, j] = jnp.dot(left, turned[s], preferred_element_type=F32).astype(BF16)
            return carry

        lax.fori_loop(0, X, ours, 0, unroll=True)

    def cross(slot, s, pown, dbuf, sbuf, rbuf):
        await_recv(dbuf.at[s], drecv.at[slot * n_seq + s])
        for d in away:
            j = (x + d) % X
            sbuf[s, d - 1] = (pown[s, j].astype(F32) + dbuf[s, j].astype(F32)).astype(BF16)
            remote(
                sbuf.at[s, d - 1], rbuf.at[s, d - 1], xsend.at[slot], xrecv.at[slot * n_seq + s], (fs, 2 * j + c)
            ).start()

    def total(slot, s, pown, dbuf, rbuf):
        await_recv(rbuf.at[s], xrecv.at[slot * n_seq + s])
        acc = pown[s, x].astype(F32) + dbuf[s, x].astype(F32)
        for d in away:
            acc = acc + rbuf[s, d - 1].astype(F32)
        return acc.T

    own_cols = span(tp * dl, dl)

    def mixer(s):
        with jax.named_scope(f"mixer#s={s}"):
            if s == 0:
                for at in range(0, 3 * dl, 256):
                    last = psum[:, at : at + 256] + plane_dot((z + Z // 2) % Z, at)
                    proj[:, at : at + 256] = last.astype(BF16)
            for at in range(0, dl, 128):
                cols = pl.ds(at, 128)
                outer = proj[seq(s), cols].astype(F32)
                inner = proj[seq(s), pl.ds(dl + at, 128)].astype(F32)
                value = proj[seq(s), pl.ds(2 * dl + at, 128)].astype(F32)
                gated[s, cols, :] = (outer * taps_of(inner * value, mtapf, cols)).T.astype(BF16)
            branch_out(0, s, gated, g12, 3 * dl, dl, ppart_m, pown_m, dbuf_m)

    def mixer_cross(s):
        with jax.named_scope(f"mcross#s={s}"):
            cross(0, s, pown_m, dbuf_m, sbuf_m, rbuf_m)

    def gather_start(s):
        with jax.named_scope(f"rs#s={s}"):
            branchw[seq(s), own_cols] = total(0, s, pown_m, dbuf_m, rbuf_m).astype(BF16)
            mine = branchw.at[seq(s), own_cols]
            for d in away:
                remote(mine, mine, agx_send, agx_recv.at[s], (fs, 2 * ((x + d) % X) + c)).start()
            remote(mine, mine, agd_send, agd_recv.at[s], (fs, partner)).start()

    def gather_share(s):
        with jax.named_scope(f"agx#s={s}"):
            await_recv(branchw.at[seq(s), pl.ds(0, (X - 1) * dl)], agx_recv.at[s])
            for d in away:
                theirs = branchw.at[seq(s), span((2 * ((x + d) % X) + c) * dl, dl)]
                remote(theirs, theirs, agd_send, agd_recv.at[s], (fs, partner)).start()

    def first_norm(s):
        with jax.named_scope(f"agd#s={s}"):
            await_recv(branchw.at[seq(s), pl.ds(0, X * dl)], agd_recv.at[s])
        with jax.named_scope(f"norm#s={s}"):
            zero = jnp.zeros((SEQ_LEN, 128), F32)

            def summed(k, acc):
                cols = span(k * 128, 128)
                v = residual_scale * tokw[seq(s), cols].astype(F32) + branchw[seq(s), cols].astype(F32)
                normed[:, cols] = v
                return acc + v

            mean = jnp.sum(lax.fori_loop(0, D // 128, summed, zero, unroll=4), axis=1, keepdims=True) * (1.0 / D)

            def squared(k, acc):
                v = normed[:, span(k * 128, 128)] - mean
                return acc + v * v

            spread = jnp.sum(lax.fori_loop(0, D // 128, squared, zero, unroll=4), axis=1, keepdims=True) * (1.0 / D)
            scale = lax.rsqrt(spread + norm_epsilon)

            def scaled(k, carry):
                cols = span(k * 128, 128)
                firstw[seq(s), cols] = ((normed[:, cols] - mean) * scale * gainw[0:1, cols]).astype(BF16)
                return carry

            lax.fori_loop(0, D // 128, scaled, 0, unroll=4)

    def ffn(s):
        with jax.named_scope(f"ffn#s={s}"):
            project(firstw, g34, seq(s), up)
            for at in range(0, fl, 128):
                cols = pl.ds(at, 128)
                left = taps_of(up[seq(s), cols].astype(F32), gtapf, cols)
                right = taps_of(up[seq(s), pl.ds(fl + at, 128)].astype(F32), vtapf, cols)
                hidden[s, cols, :] = (left / (1.0 + jnp.exp(-left)) * right).T.astype(BF16)
            branch_out(1, s, hidden, g34, 2 * fl, fl, ppart_f, pown_f, dbuf_f)

    def ffn_cross(s):
        with jax.named_scope(f"fcross#s={s}"):
            cross(1, s, pown_f, dbuf_f, sbuf_f, rbuf_f)

    lane = lax.broadcasted_iota(jnp.int32, (SEQ_LEN, 128), 1)
    line = lax.broadcasted_iota(jnp.int32, (128, SEQ_LEN), 0)

    def last_sums(s):
        with jax.named_scope(f"frs#s={s}"):
            v = residual_scale * firstw[seq(s), own_cols].astype(F32) + total(1, s, pown_f, dbuf_f, rbuf_f)
            ybuf[seq(s), :] = v
            mean = jnp.sum(v, axis=1, keepdims=True) * (1.0 / dl)
            v = v - mean
            square = jnp.sum(v * v, axis=1, keepdims=True)
            both = jnp.where(lane == 0, mean, jnp.where(lane == 1, square, 0.0))
            stats[tp, s] = both.T[:8]
            for d in range(1, TP):
                remote(stats.at[tp, s], stats.at[tp, s], st_send, st_recv.at[s], (fs, (tp + d) % TP)).start()

    def last_norm(s):
        with jax.named_scope(f"final#s={s}"):
            await_recv(stats.at[pl.ds(0, TP - 1), s], st_recv.at[s])
            theirs = stats[:, s]
            means, squares = theirs[:, 0], theirs[:, 1]
            mean = jnp.sum(means, axis=0, keepdims=True) * (1.0 / TP)
            off = means - mean
            spread = jnp.sum(squares, axis=0, keepdims=True) + dl * jnp.sum(off * off, axis=0, keepdims=True)
            scale = lax.rsqrt(spread * (1.0 / D) + norm_epsilon)
            both = jnp.where(line == 0, mean, jnp.where(line == 1, scale, 0.0)).T
            v = (ybuf[seq(s), :] - both[:, 0:1]) * both[:, 1:2]
            out_ref[seq(s), :] = (v * fgain_ref[...].astype(F32).reshape(1, dl)).astype(BF16)

    plan = [(mixer, s) for s in range(n_seq)] + [(mixer_cross, s) for s in range(n_seq)]
    plan += [(gather_start, s) for s in range(n_seq)] + [(gather_share, 0), (first_norm, 0)]
    plan += [(gather_share, s) for s in range(1, n_seq)][:1] + [(ffn, 0)]
    plan += [(gather_share, s) for s in range(2, n_seq)]
    for s in range(1, n_seq):
        plan += [(first_norm, s), (ffn_cross, s - 1), (ffn, s)]
    plan += [(ffn_cross, n_seq - 1)]
    late = ready + 1
    plan += [(last_sums, s) for s in range(n_seq)] + [(last_norm, s) for s in range(n_seq)]
    for stage, s in plan:
        while late <= ticks and (LATE_AT.get(late - ready) == (stage.__name__, s) or stage is ffn):
            late_tick(late)
            late += 1
        stage(s)

    with jax.named_scope("drain"):
        for w, g in enumerate(groups):
            await_send(g.at[pl.ds(0, Z - 1), 0], wsend.at[2 * w])
            await_send(g.at[:, pl.ds(0, Y - 1)], wsend.at[2 * w + 1])
        await_send(tokw.at[:, pl.ds(0, (TP - 1) * dl)], tok_sem.at[0])
        await_send(gainw.at[:, pl.ds(0, (TP - 1) * dl)], gain_sem.at[0])
        for slot, (ppart, sbuf) in enumerate(((ppart_m, sbuf_m), (ppart_f, sbuf_f))):
            await_send(ppart, dsend.at[slot])
            await_send(sbuf, xsend.at[slot])
        await_send(branchw.at[:, pl.ds(0, (X - 1) * dl)], agx_send)
        await_send(branchw.at[:, pl.ds(0, X * dl)], agd_send)
        await_send(stats.at[pl.ds(0, TP - 1)], st_send)


def layer(cfg, tokens, outer_gate, inner_gate, mix_value, mix_taps, mix_out, mix_gain, ffn_gate, ffn_value, gate_taps, value_taps, ffn_down, ffn_gain):
    Z, Y, TP = cfg
    X = TP // 2
    rows, dl = tokens.shape
    kr = outer_gate.shape[0]
    h = kr // 2
    fl = ffn_gate.shape[1]
    D = TP * dl
    n_seq = rows // SEQ_LEN
    vmem = pl.BlockSpec(memory_space=pltpu.VMEM)
    hbm = pl.BlockSpec(memory_space=pl.ANY)
    dma = pltpu.SemaphoreType.DMA
    exchange = [
        pltpu.VMEM((n_seq, X, dl, SEQ_LEN), BF16),
        pltpu.VMEM((n_seq, X, dl, SEQ_LEN), BF16),
        pltpu.VMEM((n_seq, X, dl, SEQ_LEN), BF16),
        pltpu.VMEM((n_seq, X - 1, dl, SEQ_LEN), BF16),
        pltpu.VMEM((n_seq, X - 1, dl, SEQ_LEN), BF16),
    ]
    return pl.pallas_call(
        functools.partial(kernel, cfg),
        out_shape=pltpu.VMEM((rows, dl), BF16),
        in_specs=[hbm, hbm, hbm, hbm, vmem, hbm, vmem, hbm, hbm, vmem, vmem, hbm, vmem],
        out_specs=vmem,
        scratch_shapes=[
            pltpu.VMEM((Z, Y, 2, h, 4 * dl), BF16),
            pltpu.VMEM((Z, Y, 2, h, 3 * fl), BF16),
            pltpu.VMEM((rows, D), BF16),
            pltpu.VMEM((8, D), F32),
            pltpu.VMEM((rows, D), BF16),
            pltpu.VMEM((rows, D), BF16),
            pltpu.VMEM((SEQ_LEN, D), F32),
            pltpu.VMEM((rows, 3 * dl), F32),
            pltpu.VMEM((rows, 3 * dl), BF16),
            pltpu.VMEM((n_seq, dl, SEQ_LEN), BF16),
            pltpu.VMEM((rows, 2 * fl), BF16),
            pltpu.VMEM((n_seq, fl, SEQ_LEN), BF16),
            *exchange,
            *exchange,
            pltpu.VMEM((rows, dl), F32),
            pltpu.VMEM((TP, n_seq, 8, SEQ_LEN), F32),
            pltpu.VMEM((3, dl), F32),
            pltpu.VMEM((3, fl), F32),
            pltpu.VMEM((3, fl), F32),
            dma((96,)),
            dma((4,)),
            dma((3,)),
            dma((2,)),
            dma((2,)),
            dma((2,)),
            dma((2 * n_seq,)),
            dma((2,)),
            dma((2 * n_seq,)),
            dma,
            dma((n_seq,)),
            dma,
            dma((n_seq,)),
            dma,
            dma((n_seq,)),
        ],
        compiler_params=pltpu.CompilerParams(
            collective_id=0, has_side_effects=True, vmem_limit_bytes=VMEM_LIMIT
        ),
    )(
        tokens,
        outer_gate,
        inner_gate,
        mix_value,
        mix_taps,
        mix_out.T,
        mix_gain,
        ffn_gate,
        ffn_value,
        gate_taps,
        value_taps,
        ffn_down.T,
        ffn_gain,
    )


def solution(mesh):
    placed = (
        P("fs", "tp"),
        P("fs", "tp"),
        P("fs", "tp"),
        P("fs", "tp"),
        P(None, "tp"),
        P("tp", "fs"),
        P("tp"),
        P("fs", "tp"),
        P("fs", "tp"),
        P(None, "tp"),
        P(None, "tp"),
        P("tp", "fs"),
        P("tp"),
    )
    cfg = (RING_Z, RING_Y, mesh.shape["tp"])
    return jax.shard_map(
        functools.partial(layer, cfg), mesh=mesh, in_specs=placed, out_specs=P("fs", "tp"), check_vma=False
    )
```

```python
import functools

import jax
import jax.numpy as jnp
from jax import lax
from jax.experimental import pallas as pl
from jax.experimental.pallas import tpu as pltpu
from jax.sharding import PartitionSpec as P

SEQ_LEN = 128
RING_Z = 8
RING_Y = 8
residual_scale = 8.0**0.25
norm_epsilon = 1e-05
MESH = pl.DeviceIdType.MESH
RIGHT, LEFT = 0, 1
W34_FIRST = 0
W34_BEGIN = 5
W34_SECOND = (5, 5, 6, 6, 6)
LATE_AT = {
    0: ("mixer_cross", 0),
    1: ("gather_start", 0),
    2: ("gather_start", 1),
    3: ("gather_share", 0),
    4: ("gather_share", 1),
}
VMEM_LIMIT = 60 * 1024 * 1024
F32 = jnp.float32
BF16 = jnp.bfloat16


def kernel(
    cfg,
    tok_ref,
    og_ref,
    ig_ref,
    mv_ref,
    mtaps_ref,
    mo_ref,
    mgain_ref,
    fg_ref,
    fv_ref,
    gtaps_ref,
    vtaps_ref,
    fd_ref,
    fgain_ref,
    out_ref,
    g12,
    g34,
    tokw,
    gainw,
    branchw,
    firstw,
    normed,
    psum,
    proj,
    gated,
    up,
    hidden,
    ppart_m,
    pown_m,
    dbuf_m,
    sbuf_m,
    rbuf_m,
    ppart_f,
    pown_f,
    dbuf_f,
    sbuf_f,
    rbuf_f,
    ybuf,
    stats,
    mtapf,
    gtapf,
    vtapf,
    wrecv,
    wsend,
    loc_sem,
    tok_sem,
    gain_sem,
    dsend,
    drecv,
    xsend,
    xrecv,
    agx_send,
    agx_recv,
    agd_send,
    agd_recv,
    st_send,
    st_recv,
):
    Z, Y, TP = cfg
    X = TP // 2
    rows, dl = tok_ref.shape
    kr = og_ref.shape[0]
    h = kr // 2
    fl = fg_ref.shape[1]
    D = TP * dl
    n_seq = rows // SEQ_LEN
    fs = lax.axis_index("fs")
    tp = lax.axis_index("tp")
    z, y = fs // Y, fs % Y
    x, c = tp // 2, tp % 2
    partner = 2 * x + (1 - c)
    groups = (g12, g34)
    away = list(dict.fromkeys([X // 2, *range(1, X)]))

    def ring_id(axis, step):
        if axis == "y":
            return (z * Y + (y + step + Y) % Y, tp)
        return (((z + step + Z) % Z) * Y + y, tp)

    def span(at, size):
        return pl.ds(pl.multiple_of(at, size), size)

    def remote(src, dst, send_sem, recv_sem, to):
        return pltpu.make_async_remote_copy(
            src_ref=src, dst_ref=dst, send_sem=send_sem, recv_sem=recv_sem, device_id=to, device_id_type=MESH
        )

    def await_recv(box, sem):
        remote(box, box, sem, sem, (fs, partner)).wait_recv()

    def await_send(box, sem):
        remote(box, box, sem, sem, (fs, partner)).wait_send()

    barrier = pltpu.get_barrier_semaphore()
    for axis in ("y", "z"):
        for step in (1, -1, 2, -2):
            pl.semaphore_signal(barrier, inc=1, device_id=ring_id(axis, step), device_id_type=MESH)
    for d in range(1, TP):
        pl.semaphore_signal(barrier, inc=1, device_id=(fs, (tp + d) % TP), device_id_type=MESH)

    def place(g, refs, sem):
        at = 0
        for ref in refs:
            cols = ref.shape[1]
            for half in range(2):
                pltpu.make_async_copy(
                    ref.at[pl.ds(half * h, h)], g.at[z, y, half, :, pl.ds(at, cols)], sem
                ).start()
            at += cols

    own_tokens = pltpu.make_async_copy(tok_ref, tokw.at[:, span(tp * dl, dl)], loc_sem.at[2])
    place(g12, (og_ref, ig_ref, mv_ref, mo_ref), loc_sem.at[0])
    own_tokens.start()
    place(g34, (fg_ref, fv_ref, fd_ref), loc_sem.at[1])
    gainw[:, span(tp * dl, dl)] = jnp.broadcast_to(mgain_ref[...].astype(F32).reshape(1, dl), (8, dl))
    mtapf[...] = mtaps_ref[...].astype(F32)
    gtapf[...] = gtaps_ref[...].astype(F32)
    vtapf[...] = vtaps_ref[...].astype(F32)

    def placed(w):
        pltpu.make_async_copy(groups[w].at[z, y], groups[w].at[z, y], loc_sem.at[w]).wait()

    placed(0)
    with jax.named_scope("greet"):
        pl.semaphore_wait(barrier, 8 + TP - 1)

    def piece(w, colour, one, two):
        return groups[w].at[two, one, 0] if colour == 0 else groups[w].at[one, two, 1]

    def rings(colour):
        return (("y", Y, y), ("z", Z, z)) if colour == 0 else (("z", Z, z), ("y", Y, y))

    def recv_sem(w, colour, kind, step):
        return wrecv.at[((w * 2 + colour) * 6 + kind) * 4 + step]

    def send_first(w, colour, step):
        (axis, n, me), (_, _, other) = rings(colour)
        for way in (RIGHT, LEFT):
            if step == n // 2 - 1 and way != w % 2:
                continue
            straight = w == 0 and step == 1 and n >= 8
            reach, back = (2, 0) if straight else (1, step)
            origin = (me - back + n) % n if way == RIGHT else (me + back) % n
            ref = piece(w, colour, origin, other)
            remote(
                ref, ref, wsend.at[2 * w], recv_sem(w, colour, 5, step), ring_id(axis, reach if way == RIGHT else -reach)
            ).start()

    def first_count(colour, step):
        return 1 if step == rings(colour)[0][1] // 2 - 1 else 2

    def members(n, g):
        return [0] if g == 0 else [g] if g == n // 2 else [g, -g]

    def halves(n, g):
        return ([0], []) if g == 0 else ([], [g]) if g == n // 2 else ([g], [-g])

    def send_second(w, colour, g, step):
        (_, n1, me1), (axis, n2, me2) = rings(colour)
        for way in (RIGHT, LEFT):
            at = members(n1, g) if step < n2 // 2 - 1 else halves(n1, g)[way]
            origin = (me2 - step + n2) % n2 if way == RIGHT else (me2 + step) % n2
            for m in at:
                ref = piece(w, colour, (me1 + m + n1) % n1, origin)
                remote(
                    ref, ref, wsend.at[2 * w + 1], recv_sem(w, colour, g, step), ring_id(axis, 1 if way == RIGHT else -1)
                ).start()

    def second_count(colour, g, step):
        n1, n2 = rings(colour)[0][1], rings(colour)[1][1]
        if step < n2 // 2 - 1:
            return 2 * len(members(n1, g))
        return sum(len(part) for part in halves(n1, g))

    def await_pieces(w, count, sem):
        g = groups[w]
        await_recv(g.at[0, 0, 0] if count == 1 else g.at[pl.ds(0, count), 0, 0], sem)

    def first_arrives(w, k):
        for colour in range(2):
            n1 = rings(colour)[0][1]
            if k < n1 // 2:
                await_pieces(w, first_count(colour, k), recv_sem(w, colour, 5, k))
                if k + 1 < n1 // 2 and (w == 1 or k > 0 or n1 < 8):
                    send_first(w, colour, k + 1)

    def second_begins(w, g):
        for colour in range(2):
            if g <= rings(colour)[0][1] // 2:
                send_second(w, colour, g, 0)

    def second_arrives(w, g, step):
        for colour in range(2):
            n1, n2 = rings(colour)[0][1], rings(colour)[1][1]
            if g <= n1 // 2 and step < n2 // 2:
                await_pieces(w, second_count(colour, g, step), recv_sem(w, colour, g, step))
                if step + 1 < n2 // 2:
                    send_second(w, colour, g, step + 1)

    most = max(Y, Z) // 2
    first_tick = {(0, k): max(0, k - 1) if most >= 4 else k for k in range(most)}
    first_tick.update({(1, k): W34_FIRST + 1 + k for k in range(most)})
    second_tick = {(0, g): first_tick[0, g - 1] if g > 0 else -1 for g in range(most + 1)}
    for g in range(most + 1):
        second_tick[1, g] = max(W34_SECOND[min(g, 4)], first_tick[1, g - 1] if g > 0 else 0)
    begin_tick = {g: max(W34_BEGIN, first_tick[1, g - 1] if g > 0 else 0) for g in range(most + 1)}
    for g in range(most + 1):
        second_tick[1, g] = max(second_tick[1, g], begin_tick[g])
    ready = max(second_tick[0, g] for g in range(most + 1)) + most
    ticks = max(second_tick[1, g] for g in range(most + 1)) + most

    def tick(at, which=(0, 1)):
        for w in which:
            firsts = [k for k in range(most) if first_tick[w, k] == at]
            for k in firsts[:1]:
                first_arrives(w, k)
                if w == 0:
                    second_begins(w, k + 1)
            for step in range(most):
                for g in range(most + 1):
                    if second_tick[w, g] + 1 + step == at:
                        second_arrives(w, g, step)
            for k in firsts[1:]:
                first_arrives(w, k)
                if w == 0:
                    second_begins(w, k + 1)
            if w == 1:
                if at == W34_FIRST:
                    placed(1)
                    for colour in range(2):
                        send_first(1, colour, 0)
                for g in range(most + 1):
                    if begin_tick[g] == at:
                        second_begins(1, g)

    def late_tick(k):
        with jax.named_scope(f"late#k={k}"):
            tick(k, (1,))

    for colour in range(2):
        send_first(0, colour, 0)
    second_begins(0, 0)
    for colour in range(2):
        if rings(colour)[0][1] >= 8:
            send_first(0, colour, 1)
    own_tokens.wait()
    mine = tokw.at[:, span(tp * dl, dl)]
    for d in range(1, TP):
        remote(mine, mine, tok_sem.at[0], tok_sem.at[1], (fs, (tp + d) % TP)).start()
    mine = gainw.at[:, span(tp * dl, dl)]
    for d in range(1, TP):
        remote(mine, mine, gain_sem.at[0], gain_sem.at[1], (fs, (tp + d) % TP)).start()
    for k in range(ready):
        with jax.named_scope(f"early#k={k}"):
            tick(k)
    with jax.named_scope("tokens"):
        await_recv(tokw.at[:, pl.ds(0, (TP - 1) * dl)], tok_sem.at[1])
        await_recv(gainw.at[:, pl.ds(0, (TP - 1) * dl)], gain_sem.at[1])

    deep = D // Z

    def plane_dot(plane, at):
        right = g12[plane, :, :, :, pl.ds(at, 256)].reshape(deep, 256)
        return jnp.dot(tokw[:, span(plane * deep, deep)], right, preferred_element_type=F32)

    with jax.named_scope("planes"):
        for at in range(0, 3 * dl, 256):
            psum[:, at : at + 256] = plane_dot((z + Z // 2 + 1) % Z, at)

        def add_plane(i, carry):
            for at in range(0, 3 * dl, 256):
                psum[:, at : at + 256] += plane_dot((z + Z // 2 + i) % Z, at)
            return carry

        lax.fori_loop(2, Z, add_plane, 0)
    with jax.named_scope(f"early#k={ready}"):
        tick(ready, (0,))

    def taps_of(v, tap_ref, cols):
        at = lax.broadcasted_iota(jnp.int32, v.shape, 0)
        one = jnp.where(at >= 1, pltpu.roll(v, 1, 0), 0.0)
        two = jnp.where(at >= 2, pltpu.roll(v, 2, 0), 0.0)
        return v * tap_ref[2:3, cols] + one * tap_ref[1:2, cols] + two * tap_ref[0:1, cols]

    def seq(s):
        return pl.ds(s * SEQ_LEN, SEQ_LEN)

    def project(left, g, r, target):
        def one(n, carry):
            at = pl.multiple_of(n * 256, 256)
            right = g[:, :, :, :, pl.ds(at, 256)].reshape(D, 256)
            target[r, pl.ds(at, 256)] = jnp.dot(left[r, :], right, preferred_element_type=F32).astype(BF16)
            return carry

        lax.fori_loop(0, target.shape[1] // 256, one, 0)

    def branch_out(slot, s, turned, g, first_col, cols, ppart, pown, dbuf):
        def theirs(j, carry):
            left = g[2 * j + 1 - c, :, :, :, first_col : first_col + cols].reshape(dl, cols)
            ppart[s, j] = jnp.dot(left, turned[s], preferred_element_type=F32).astype(BF16)
            return carry

        lax.fori_loop(0, X, theirs, 0, unroll=True)
        remote(ppart.at[s], dbuf.at[s], dsend.at[slot], drecv.at[slot * n_seq + s], (fs, partner)).start()

        def ours(j, carry):
            left = g[2 * j + c, :, :, :, first_col : first_col + cols].reshape(dl, cols)
            pown[s, j] = jnp.dot(left, turned[s], preferred_element_type=F32).astype(BF16)
            return carry

        lax.fori_loop(0, X, ours, 0, unroll=True)

    def cross(slot, s, pown, dbuf, sbuf, rbuf):
        await_recv(dbuf.at[s], drecv.at[slot * n_seq + s])
        for d in away:
            j = (x + d) % X
            sbuf[s, d - 1] = (pown[s, j].astype(F32) + dbuf[s, j].astype(F32)).astype(BF16)
            remote(
                sbuf.at[s, d - 1], rbuf.at[s, d - 1], xsend.at[slot], xrecv.at[slot * n_seq + s], (fs, 2 * j + c)
            ).start()

    def total(slot, s, pown, dbuf, rbuf):
        await_recv(rbuf.at[s], xrecv.at[slot * n_seq + s])
        acc = pown[s, x].astype(F32) + dbuf[s, x].astype(F32)
        for d in away:
            acc = acc + rbuf[s, d - 1].astype(F32)
        return acc.T

    own_cols = span(tp * dl, dl)

    def mixer(s):
        with jax.named_scope(f"mixer#s={s}"):
            if s == 0:
                for at in range(0, 3 * dl, 256):
                    last = psum[:, at : at + 256] + plane_dot((z + Z // 2) % Z, at)
                    proj[:, at : at + 256] = last.astype(BF16)
            for at in range(0, dl, 128):
                cols = pl.ds(at, 128)
                outer = proj[seq(s), cols].astype(F32)
                inner = proj[seq(s), pl.ds(dl + at, 128)].astype(F32)
                value = proj[seq(s), pl.ds(2 * dl + at, 128)].astype(F32)
                gated[s, cols, :] = (outer * taps_of(inner * value, mtapf, cols)).T.astype(BF16)
            branch_out(0, s, gated, g12, 3 * dl, dl, ppart_m, pown_m, dbuf_m)

    def mixer_cross(s):
        with jax.named_scope(f"mcross#s={s}"):
            cross(0, s, pown_m, dbuf_m, sbuf_m, rbuf_m)

    def gather_start(s):
        with jax.named_scope(f"rs#s={s}"):
            branchw[seq(s), own_cols] = total(0, s, pown_m, dbuf_m, rbuf_m).astype(BF16)
            mine = branchw.at[seq(s), own_cols]
            for d in away:
                remote(mine, mine, agx_send, agx_recv.at[s], (fs, 2 * ((x + d) % X) + c)).start()
            remote(mine, mine, agd_send, agd_recv.at[s], (fs, partner)).start()

    def gather_share(s):
        with jax.named_scope(f"agx#s={s}"):
            await_recv(branchw.at[seq(s), pl.ds(0, (X - 1) * dl)], agx_recv.at[s])
            for d in away:
                theirs = branchw.at[seq(s), span((2 * ((x + d) % X) + c) * dl, dl)]
                remote(theirs, theirs, agd_send, agd_recv.at[s], (fs, partner)).start()

    def first_norm(s):
        with jax.named_scope(f"agd#s={s}"):
            await_recv(branchw.at[seq(s), pl.ds(0, X * dl)], agd_recv.at[s])
        with jax.named_scope(f"norm#s={s}"):
            zero = jnp.zeros((SEQ_LEN, 128), F32)

            def summed(k, acc):
                cols = span(k * 128, 128)
                v = residual_scale * tokw[seq(s), cols].astype(F32) + branchw[seq(s), cols].astype(F32)
                normed[:, cols] = v
                return acc + v

            mean = jnp.sum(lax.fori_loop(0, D // 128, summed, zero, unroll=4), axis=1, keepdims=True) * (1.0 / D)

            def squared(k, acc):
                v = normed[:, span(k * 128, 128)] - mean
                return acc + v * v

            spread = jnp.sum(lax.fori_loop(0, D // 128, squared, zero, unroll=4), axis=1, keepdims=True) * (1.0 / D)
            scale = lax.rsqrt(spread + norm_epsilon)

            def scaled(k, carry):
                cols = span(k * 128, 128)
                firstw[seq(s), cols] = ((normed[:, cols] - mean) * scale * gainw[0:1, cols]).astype(BF16)
                return carry

            lax.fori_loop(0, D // 128, scaled, 0, unroll=4)

    def ffn(s):
        with jax.named_scope(f"ffn#s={s}"):
            project(firstw, g34, seq(s), up)
            for at in range(0, fl, 128):
                cols = pl.ds(at, 128)
                left = taps_of(up[seq(s), cols].astype(F32), gtapf, cols)
                right = taps_of(up[seq(s), pl.ds(fl + at, 128)].astype(F32), vtapf, cols)
                hidden[s, cols, :] = (left / (1.0 + jnp.exp(-left)) * right).T.astype(BF16)
            branch_out(1, s, hidden, g34, 2 * fl, fl, ppart_f, pown_f, dbuf_f)

    def ffn_cross(s):
        with jax.named_scope(f"fcross#s={s}"):
            cross(1, s, pown_f, dbuf_f, sbuf_f, rbuf_f)

    lane = lax.broadcasted_iota(jnp.int32, (SEQ_LEN, 128), 1)
    line = lax.broadcasted_iota(jnp.int32, (128, SEQ_LEN), 0)

    def last_sums(s):
        with jax.named_scope(f"frs#s={s}"):
            v = residual_scale * firstw[seq(s), own_cols].astype(F32) + total(1, s, pown_f, dbuf_f, rbuf_f)
            ybuf[seq(s), :] = v
            mean = jnp.sum(v, axis=1, keepdims=True) * (1.0 / dl)
            v = v - mean
            square = jnp.sum(v * v, axis=1, keepdims=True)
            both = jnp.where(lane == 0, mean, jnp.where(lane == 1, square, 0.0))
            stats[tp, s] = both.T[:8]
            for d in range(1, TP):
                remote(stats.at[tp, s], stats.at[tp, s], st_send, st_recv.at[s], (fs, (tp + d) % TP)).start()

    def last_norm(s):
        with jax.named_scope(f"final#s={s}"):
            await_recv(stats.at[pl.ds(0, TP - 1), s], st_recv.at[s])
            theirs = stats[:, s]
            means, squares = theirs[:, 0], theirs[:, 1]
            mean = jnp.sum(means, axis=0, keepdims=True) * (1.0 / TP)
            off = means - mean
            spread = jnp.sum(squares, axis=0, keepdims=True) + dl * jnp.sum(off * off, axis=0, keepdims=True)
            scale = lax.rsqrt(spread * (1.0 / D) + norm_epsilon)
            both = jnp.where(line == 0, mean, jnp.where(line == 1, scale, 0.0)).T
            v = (ybuf[seq(s), :] - both[:, 0:1]) * both[:, 1:2]
            out_ref[seq(s), :] = (v * fgain_ref[...].astype(F32).reshape(1, dl)).astype(BF16)

    plan = [(mixer, s) for s in range(n_seq)] + [(mixer_cross, s) for s in range(n_seq)]
    plan += [(gather_start, s) for s in range(n_seq)] + [(gather_share, 0), (first_norm, 0)]
    plan += [(gather_share, s) for s in range(1, n_seq)][:1] + [(ffn, 0)]
    plan += [(gather_share, s) for s in range(2, n_seq)]
    for s in range(1, n_seq):
        plan += [(first_norm, s), (ffn_cross, s - 1), (ffn, s)]
    plan += [(ffn_cross, n_seq - 1)]
    late = ready
    plan += [(last_sums, s) for s in range(n_seq)] + [(last_norm, s) for s in range(n_seq)]
    for stage, s in plan:
        while late <= ticks and (LATE_AT.get(late - ready) == (stage.__name__, s) or stage is ffn):
            late_tick(late)
            late += 1
        stage(s)

    with jax.named_scope("drain"):
        for w, g in enumerate(groups):
            await_send(g.at[pl.ds(0, Z - 1), 0], wsend.at[2 * w])
            await_send(g.at[:, pl.ds(0, Y - 1)], wsend.at[2 * w + 1])
        await_send(tokw.at[:, pl.ds(0, (TP - 1) * dl)], tok_sem.at[0])
        await_send(gainw.at[:, pl.ds(0, (TP - 1) * dl)], gain_sem.at[0])
        for slot, (ppart, sbuf) in enumerate(((ppart_m, sbuf_m), (ppart_f, sbuf_f))):
            await_send(ppart, dsend.at[slot])
            await_send(sbuf, xsend.at[slot])
        await_send(branchw.at[:, pl.ds(0, (X - 1) * dl)], agx_send)
        await_send(branchw.at[:, pl.ds(0, X * dl)], agd_send)
        await_send(stats.at[pl.ds(0, TP - 1)], st_send)


def layer(cfg, tokens, outer_gate, inner_gate, mix_value, mix_taps, mix_out, mix_gain, ffn_gate, ffn_value, gate_taps, value_taps, ffn_down, ffn_gain):
    Z, Y, TP = cfg
    X = TP // 2
    rows, dl = tokens.shape
    kr = outer_gate.shape[0]
    h = kr // 2
    fl = ffn_gate.shape[1]
    D = TP * dl
    n_seq = rows // SEQ_LEN
    vmem = pl.BlockSpec(memory_space=pltpu.VMEM)
    hbm = pl.BlockSpec(memory_space=pl.ANY)
    dma = pltpu.SemaphoreType.DMA
    exchange = [
        pltpu.VMEM((n_seq, X, dl, SEQ_LEN), BF16),
        pltpu.VMEM((n_seq, X, dl, SEQ_LEN), BF16),
        pltpu.VMEM((n_seq, X, dl, SEQ_LEN), BF16),
        pltpu.VMEM((n_seq, X - 1, dl, SEQ_LEN), BF16),
        pltpu.VMEM((n_seq, X - 1, dl, SEQ_LEN), BF16),
    ]
    return pl.pallas_call(
        functools.partial(kernel, cfg),
        out_shape=pltpu.VMEM((rows, dl), BF16),
        in_specs=[hbm, hbm, hbm, hbm, vmem, hbm, vmem, hbm, hbm, vmem, vmem, hbm, vmem],
        out_specs=vmem,
        scratch_shapes=[
            pltpu.VMEM((Z, Y, 2, h, 4 * dl), BF16),
            pltpu.VMEM((Z, Y, 2, h, 3 * fl), BF16),
            pltpu.VMEM((rows, D), BF16),
            pltpu.VMEM((8, D), F32),
            pltpu.VMEM((rows, D), BF16),
            pltpu.VMEM((rows, D), BF16),
            pltpu.VMEM((SEQ_LEN, D), F32),
            pltpu.VMEM((rows, 3 * dl), F32),
            pltpu.VMEM((rows, 3 * dl), BF16),
            pltpu.VMEM((n_seq, dl, SEQ_LEN), BF16),
            pltpu.VMEM((rows, 2 * fl), BF16),
            pltpu.VMEM((n_seq, fl, SEQ_LEN), BF16),
            *exchange,
            *exchange,
            pltpu.VMEM((rows, dl), F32),
            pltpu.VMEM((TP, n_seq, 8, SEQ_LEN), F32),
            pltpu.VMEM((3, dl), F32),
            pltpu.VMEM((3, fl), F32),
            pltpu.VMEM((3, fl), F32),
            dma((96,)),
            dma((4,)),
            dma((3,)),
            dma((2,)),
            dma((2,)),
            dma((2,)),
            dma((2 * n_seq,)),
            dma((2,)),
            dma((2 * n_seq,)),
            dma,
            dma((n_seq,)),
            dma,
            dma((n_seq,)),
            dma,
            dma((n_seq,)),
        ],
        compiler_params=pltpu.CompilerParams(
            collective_id=0, has_side_effects=True, vmem_limit_bytes=VMEM_LIMIT
        ),
    )(
        tokens,
        outer_gate,
        inner_gate,
        mix_value,
        mix_taps,
        mix_out.T,
        mix_gain,
        ffn_gate,
        ffn_value,
        gate_taps,
        value_taps,
        ffn_down.T,
        ffn_gain,
    )


def solution(mesh):
    placed = (
        P("fs", "tp"),
        P("fs", "tp"),
        P("fs", "tp"),
        P("fs", "tp"),
        P(None, "tp"),
        P("tp", "fs"),
        P("tp"),
        P("fs", "tp"),
        P("fs", "tp"),
        P(None, "tp"),
        P(None, "tp"),
        P("tp", "fs"),
        P("tp"),
    )
    cfg = (RING_Z, RING_Y, mesh.shape["tp"])
    return jax.shard_map(
        functools.partial(layer, cfg), mesh=mesh, in_specs=placed, out_specs=P("fs", "tp"), check_vma=False
    )
```
